32 devices in a mesh: grp: 2 (over x), fs: 4 (over z), tp: 4 (over y, core).
Axes of the slice: x: 2, y: 2, z: 4, core: 2. Of those that a mesh axis runs over, the one named last changes fastest.
Arguments:
- tokens: bfloat16 [4096, 2048], P(('grp', 'fs')), parts along dimension 0, may hold values from -200 to 200
- norm_gain: float32 [2048], replicated, may hold values from 0.1 to 1.9
- value_weight: float32 [2048, 5632], P('fs', 'tp'), may hold values from -0.125 to 0.125
- gate_weight: float32 [2048, 5632], P('fs', 'tp'), may hold values from -0.125 to 0.125
- down_weight: float32 [2048, 5632], P('fs', 'tp'), may hold values from -0.078125 to 0.078125
- value_scale: float32 [5632], P('tp'), may hold values from 0.3 to 3
- gate_scale: float32 [5632], P('tp'), may hold values from 0.3 to 3
- down_scale: float32 [2048], replicated, may hold values from 0.3 to 3
- value_taps: float32 [3, 5632], P(None, 'tp'), may hold values from -3 to 3
- gate_taps: float32 [3, 5632], P(None, 'tp'), may hold values from -3 to 3
- value_bias: float32 [5632], P('tp'), may hold values from -3 to 3
- gate_bias: float32 [5632], P('tp'), may hold values from -3 to 3
Outputs:
- mixed: bfloat16 [4096, 2048], P(('grp', 'fs', 'tp')), parts along dimension 0
The draws below stay inside these ranges and needn't reach their ends.
There are 2 independent parts, one for each index of `grp`. The reference program is written for one: setup_inputs(seed, part) draws one part's arguments, and reference() takes and returns one part's arrays. A program takes and returns all parts, laid end to end along the dimension named above; an argument that names none is the same for every part. Nothing has to cross between parts.
All inputs are finite; a program needn't handle non-finite values.
Results may differ from the reference program's by a relative error of at most 0.024.
Values may be sent and summed in bfloat16 or wider, within the bound.
A program may use at most 64 MiB of HBM per device.

```python
import math
import jax
import jax.numpy as jnp
from jax import lax

D = 2048
FF = 5632
TAPS = 3
ROWS = 512
TOKENS = 2048
N_FS = 4
N_TP = 4


def draw_tokens(key, part):
    key_base = jax.random.fold_in(key, 11)
    key_rows = jax.random.fold_in(key, 12)
    base = jnp.clip(jax.random.normal(key_base, (TOKENS, D), jnp.float32), -6.0, 6.0)
    spread = jax.random.uniform(key_rows, (TOKENS, 1), jnp.float32, 0.0, math.log(10.0))
    return (base * jnp.exp(spread)).astype(jnp.bfloat16)


def levels(rng, shape, split, smallest, high):
    def one(position, shards_of):
        steps = jax.random.uniform(jax.random.fold_in(jax.random.fold_in(rng, 6), position), (shards_of,), jnp.float32, smallest / len(split), high / len(split))
        return jnp.repeat(jnp.exp(steps), shape[position] // shards_of).reshape((-1,) + (1,) * (len(shape) - position - 1))

    level = one(*split[0])
    for cut in split[1:]:
        level = level * one(*cut)
    return level


def scatter_about(rng, extent, scale, reach, shards=(), kind=jnp.bfloat16):
    drawn = scale * jax.random.normal(rng, extent, jnp.float32)
    if shards:
        drawn = drawn * levels(rng, extent, shards, -0.22, 0.18)
    return jnp.clip(drawn, -reach, reach).astype(kind)


def setup_inputs(seed: int = 0, part: int = 0) -> dict:
    keys = jax.random.split(jax.random.key(seed), 13)
    part_keys = jax.random.split(jax.random.fold_in(keys[12], part), 13)
    tokens = draw_tokens(jax.random.fold_in(jax.random.fold_in(keys[12], part), 71), part)
    norm_gain = jnp.clip(1.0 + 0.18 * jax.random.normal(keys[1], (D,), jnp.float32), 0.1, 1.9)
    value_weight = scatter_about(keys[2], (D, FF), D ** -0.5, 0.125, ((0, 4), (1, 4)), jnp.float32)
    gate_weight = scatter_about(keys[3], (D, FF), D ** -0.5, 0.125, ((0, 4), (1, 4)), jnp.float32)
    down_weight = scatter_about(keys[4], (D, FF), FF ** -0.5, 0.078125, ((0, 4), (1, 4)), jnp.float32)
    value_scale = jnp.clip(jnp.exp(math.log(3.0) - 2.3025851 * jax.random.uniform(keys[5], (FF,), jnp.float32) ** levels(keys[5], (FF,), ((0, 4),), -0.2, 0.2)), 0.3, 3.0)
    gate_scale = jnp.clip(jnp.exp(math.log(3.0) - 2.3025851 * jax.random.uniform(keys[6], (FF,), jnp.float32) ** levels(keys[6], (FF,), ((0, 4),), -0.2, 0.2)), 0.3, 3.0)
    down_scale = jnp.clip(jnp.exp(jax.random.uniform(keys[7], (D,), jnp.float32, math.log(0.3), math.log(3.0))), 0.3, 3.0)
    value_taps = scatter_about(keys[8], (TAPS, FF), 0.577, 3.0, ((1, 4),), jnp.float32)
    gate_taps = scatter_about(keys[9], (TAPS, FF), 0.577, 3.0, ((1, 4),), jnp.float32)
    value_bias = scatter_about(keys[10], (FF,), 0.5, 3.0, ((0, 4),), jnp.float32)
    gate_bias = scatter_about(keys[11], (FF,), 0.5, 3.0, ((0, 4),), jnp.float32)
    return dict(tokens=tokens, norm_gain=norm_gain, value_weight=value_weight, gate_weight=gate_weight, down_weight=down_weight, value_scale=value_scale, gate_scale=gate_scale, down_scale=down_scale, value_taps=value_taps, gate_taps=gate_taps, value_bias=value_bias, gate_bias=gate_bias)


def causal_mix(field, taps, bias):
    back_one = jnp.pad(field, ((1, 0), (0, 0)))[:-1]
    back_two = jnp.pad(field, ((2, 0), (0, 0)))[:-2]
    return taps[0] * back_two + taps[1] * back_one + taps[2] * field + bias

def reference(tokens, norm_gain, value_weight, gate_weight, down_weight, value_scale, gate_scale, down_scale, value_taps, gate_taps, value_bias, gate_bias):
    value_cast = value_weight.astype(jnp.bfloat16)
    gate_cast = gate_weight.astype(jnp.bfloat16)
    down_cast = down_weight.astype(jnp.bfloat16)

    def one_sequence(rows):
        floated = rows.astype(jnp.float32)
        inverse = lax.rsqrt(lax.optimization_barrier(jnp.mean(floated * floated, axis=-1, keepdims=True)) + 1e-06)
        normed = (floated * inverse * norm_gain).astype(jnp.bfloat16)
        value_up = jnp.dot(normed, value_cast, preferred_element_type=jnp.float32) * value_scale
        gate_up = jnp.dot(normed, gate_cast, preferred_element_type=jnp.float32) * gate_scale
        value_mixed = causal_mix(value_up, value_taps, value_bias)
        gate_mixed = causal_mix(gate_up, gate_taps, gate_bias)
        return (jax.nn.silu(gate_mixed) * value_mixed).astype(jnp.bfloat16)
    hidden = lax.map(one_sequence, tokens.reshape(N_FS, ROWS, D)).reshape(N_FS * ROWS, FF)
    block = FF // N_TP

    def add_block(index, total):
        start = (index * block).astype(jnp.int32)
        left = lax.dynamic_slice_in_dim(hidden, start, block, 1)
        right = lax.dynamic_slice_in_dim(down_cast, start, block, 1)
        term = lax.dot_general(left, right, (((1,), (1,)), ((), ())), preferred_element_type=jnp.float32)
        return total + term.astype(jnp.bfloat16).astype(jnp.float32)
    total = lax.fori_loop(0, N_TP, add_block, jnp.zeros((N_FS * ROWS, D), jnp.float32))
    return (total * down_scale).astype(jnp.bfloat16)
```

```python
import functools

import jax
import jax.numpy as jnp
from jax import lax
from jax.experimental import pallas as pl
from jax.experimental.pallas import tpu as pltpu
from jax.sharding import PartitionSpec as P

MESH = pl.DeviceIdType.MESH
WIDE = 256
CUT = 2


def kernel(
    parts,
    line,
    peers,
    lent,
    tokens,
    norm_gain,
    value_weight,
    gate_weight,
    down_weight,
    value_scale,
    gate_scale,
    down_scale,
    value_taps,
    gate_taps,
    value_bias,
    gate_bias,
    out,
    *scratch,
):
    group, here, me = lax.axis_index("grp"), lax.axis_index("fs"), lax.axis_index("tp")
    scratch = list(scratch)
    take = lambda count: [scratch.pop(0) for _ in range(count)]
    kinds = 2 if lent else 1
    rows, width = tokens.shape
    held, units = value_weight.shape
    kept = rows // peers
    pairs = peers // parts
    base = (0, units - lent)
    span = (units - lent, lent)
    many = [span[k] // WIDE for k in range(kinds)]
    left_over = [span[k] % WIDE for k in range(kinds)]
    wide = [take(1)[0] if many[k] else None for k in range(kinds)]
    rest = [take(1)[0] if left_over[k] else None for k in range(kinds)]
    down = take(kinds)
    hidden = take(kinds)
    raw, normed, along, gains, partial, landed = take(6)
    send_sem, recv_sem, token_sem, along_sem, sum_send, sum_recv = take(6)
    if lent:
        guest, guest_normed, guest_hidden, guest_partial, guest_landed, summed, returned = take(7)
        guest_send, guest_recv, guest_sum_send, guest_sum_recv, back_send, back_recv = take(6)

    pair = lax.div(me, parts)
    core = lax.rem(me, parts)
    boss = core == group
    other = jnp.logical_not(boss)
    block = pair * parts + group
    sibling = pair * parts + lax.rem(core + 1, parts)
    end = jnp.logical_or(here == 0, here == line - 1)
    inner = jnp.logical_not(end)
    helper = jnp.logical_and(inner, jnp.logical_or(here == 1, here == line - 2))
    mate = jnp.where(end, jnp.where(here == 0, 1, line - 2), jnp.where(here == 1, 0, line - 1))
    both = jnp.logical_and

    barrier = pltpu.get_barrier_semaphore()

    def greet(target):
        pl.semaphore_signal(barrier, inc=1, device_id=target, device_id_type=MESH)

    pl.when(here > 0)(lambda: greet({"fs": here - 1}))
    pl.when(here < line - 1)(lambda: greet({"fs": here + 1}))
    for j in range(parts):
        for k in range(peers):
            if j or k:
                greet({"grp": lax.rem(group + j, parts), "tp": lax.rem(me + k, peers)})

    def owner_at(i):
        near = jnp.where(here < line // 2, here, line - 1 - here)
        turned = jnp.where(i % 2 == 1, near - (i + 1) // 2, near + i // 2)
        first = jnp.where(i > 2 * near, i, turned)
        return jnp.where(here < line // 2, first, line - 1 - first)

    numbers = {}
    count = 0
    for k in range(kinds):
        for name, amount in (("wide", many[k]), ("rest", 1 if left_over[k] else 0), ("down", 1)):
            numbers[name, k] = count
            count += amount * CUT

    def piece(name, kind, q, r):
        number = numbers[name, kind] + q * CUT + r

        def ref(owner):
            part = held // CUT
            first = pl.multiple_of(owner * held + r * part, part)
            if name == "wide":
                return wide[kind].at[q, :, pl.ds(first, part), :]
            if name == "rest":
                return rest[kind].at[:, pl.ds(first, part), :]
            return down[kind].at[pl.ds(first, part), :]

        return number, kind, ref

    def groups(kind, body):
        if many[kind]:

            def one(q, carry):
                body("wide", q)
                return carry

            lax.fori_loop(0, many[kind], one, 0)
        if left_over[kind]:
            body("rest", 0)

    def copy(which, owner, direction):
        number, kind, ref = which
        if direction is None:
            target, lane = {"tp": sibling}, 2
        else:
            target = {"fs": lax.clamp(0, here + direction, line - 1)}
            lane = jnp.where(direction > 0, 0, 1)
        return pltpu.make_async_remote_copy(
            src_ref=ref(owner),
            dst_ref=ref(owner),
            send_sem=send_sem.at[number, owner, lane],
            recv_sem=recv_sem.at[number, owner],
            device_id=target,
            device_id_type=MESH,
        )

    def used(kind):
        return inner if kind else here >= 0

    def further(kind, direction):
        there = here + direction
        return both(there >= kind, there <= line - 1 - kind)

    def start(dma):
        dma.start()

    def left(dma):
        dma.wait_send()

    def toward_end(direction):
        there = here + direction
        return jnp.logical_or(end, jnp.logical_or(there == 0, there == line - 1))

    def own_line(which, act, early=None):
        for direction in (1, -1):
            go = both(boss, further(which[1], direction))
            if early is True:
                go = both(go, toward_end(direction))
            elif early is False:
                go = both(go, jnp.logical_not(toward_end(direction)))
            pl.when(go)(lambda: act(copy(which, here, direction)))

    def own_across(which, act):
        pl.when(both(boss, used(which[1])))(lambda: act(copy(which, here, None)))

    def onward(which, owner, act, arrive):
        direction = jnp.where(owner < here, 1, -1)

        @pl.when(used(which[1]))
        def _():
            if arrive:
                copy(which, owner, None).wait_recv()

            @pl.when(boss)
            def _():
                pl.when(further(which[1], direction))(lambda: act(copy(which, owner, direction)))
                act(copy(which, owner, None))

    def arrive(which, owner):
        onward(which, owner, start, True)

    def at_home(which):
        pl.when(both(other, used(which[1])))(lambda: copy(which, here, None).wait_recv())

    def pieces_up(kind, body):
        def group_body(name, q):
            for r in range(CUT):
                body(piece(name, kind, q, r))

        groups(kind, group_body)

    def pieces_down(kind, body):
        for r in range(CUT):
            body(piece("down", kind, 0, r))

    def cast_rows(source, columns, store):
        step = min(held, 64)

        def body(i, carry):
            taken = pl.ds(pl.multiple_of(i * step, step), step)
            target = pl.ds(pl.multiple_of(here * held + i * step, step), step)
            store(target, source[taken, columns].astype(jnp.bfloat16))
            return carry

        lax.fori_loop(0, held // step, body, 0)

    def cast_up(kind):
        for m, source in enumerate((value_weight, gate_weight)):
            for q in range(many[kind]):
                first = base[kind] + q * WIDE

                def store(target, values):
                    wide[kind][q, m, target, :] = values

                cast_rows(source, slice(first, first + WIDE), store)
            if left_over[kind]:
                first = base[kind] + many[kind] * WIDE

                def store(target, values):
                    rest[kind][m, target, :] = values

                cast_rows(source, slice(first, first + left_over[kind]), store)

    def cast_down(kind):
        def store(target, values):
            down[kind][target, :] = values

        cast_rows(down_weight, slice(base[kind], base[kind] + span[kind]), store)

    def normalize(source, target):
        step = min(rows, 64)

        def body(i, carry):
            taken = pl.ds(pl.multiple_of(i * step, step), step)
            floated = source[taken, :].astype(jnp.float32)
            mean = jnp.mean(floated * floated, axis=-1, keepdims=True)
            target[taken, :] = (floated * lax.rsqrt(mean + 1e-06) * gains[0:1, :]).astype(
                jnp.bfloat16
            )
            return carry

        lax.fori_loop(0, rows // step, body, 0)

    def swap():
        return pltpu.make_async_remote_copy(
            src_ref=tokens,
            dst_ref=raw,
            send_sem=token_sem.at[0],
            recv_sem=token_sem.at[1],
            device_id={"grp": lax.rem(group + 1, parts)},
            device_id_type=MESH,
        )

    def vectors():
        return pltpu.make_async_remote_copy(
            src_ref=along,
            dst_ref=along,
            send_sem=along_sem.at[0],
            recv_sem=along_sem.at[1],
            device_id={"tp": sibling},
            device_id_type=MESH,
        )

    share = rows // pairs

    def portion(ref):
        return ref.at[pl.ds(pl.multiple_of(pair * share, share), share), :]

    def guest_copy(source, slot, target):
        return pltpu.make_async_remote_copy(
            src_ref=portion(source),
            dst_ref=portion(guest),
            send_sem=guest_send.at[slot],
            recv_sem=guest_recv.at[pair],
            device_id=target,
            device_id_type=MESH,
        )

    def lend():
        return guest_copy(tokens, pairs, {"fs": mate})

    def pass_on(k):
        return guest_copy(guest, k, {"tp": lax.rem(me + k * parts, peers)})

    def pass_across():
        return guest_copy(guest, 0, {"grp": lax.rem(group + 1, parts)})

    def relay():
        lend().wait_recv()
        pl.when(boss)(lambda: pass_across().start())
        for k in range(1, pairs):
            pass_on(k).start()

    def welcome():
        for k in range(1, pairs):
            from_pair = lax.rem(pair + k, pairs)
            landed_share = guest.at[pl.ds(pl.multiple_of(from_pair * share, share), share), :]
            pltpu.make_async_copy(landed_share, landed_share, guest_recv.at[from_pair]).wait()
        normalize(guest, guest_normed)

    def causal(weight, tap, bias, source, outer):
        up = jnp.dot(source[...], weight[...], preferred_element_type=jnp.float32)
        position = lax.broadcasted_iota(jnp.int32, up.shape, 0)
        one = jnp.where(position >= 1, pltpu.roll(up, 1, axis=0), 0.0)
        two = jnp.where(position >= 2, pltpu.roll(up, 2, axis=0), 0.0)
        return (
            along[tap : tap + 1, outer] * two
            + along[tap + 1 : tap + 2, outer] * one
            + along[tap + 2 : tap + 3, outer] * up
            + along[bias : bias + 1, outer]
        )

    def up(kind, name, q, source, keep):
        weights = wide[kind].at[q] if name == "wide" else rest[kind]
        extent = WIDE if name == "wide" else left_over[kind]
        first = q * WIDE if name == "wide" else many[kind] * WIDE
        if name == "wide":
            first = pl.multiple_of(first, WIDE)
            outer = pl.ds(pl.multiple_of(base[kind] + first, 128), extent)
        else:
            outer = pl.ds(base[kind] + first, extent)
        value = causal(weights.at[0], 0, 6, source, outer)
        gate = causal(weights.at[1], 3, 7, source, outer)
        keep[:, pl.ds(first, extent)] = (gate / (1.0 + jnp.exp(-gate)) * value).astype(jnp.bfloat16)

    def through(kind, activations, owner):
        shard = down[kind][pl.ds(pl.multiple_of(owner * held, held), held), :]
        return lax.dot_general(
            activations[...], shard, (((1,), (1,)), ((), ())), preferred_element_type=jnp.float32
        )

    def hand(source, target, owner, k, sent, received):
        peer = lax.rem(me + k, peers)
        return pltpu.make_async_remote_copy(
            src_ref=source.at[owner, pl.ds(pl.multiple_of(peer * kept, kept), kept), :],
            dst_ref=target.at[owner, block],
            send_sem=sent,
            recv_sem=received.at[owner],
            device_id={"grp": core, "tp": peer},
            device_id_type=MESH,
        )

    def hand_out(source, target, owner, sent, received):
        pl.when(other)(lambda: hand(source, target, owner, 0, sent, received).start())
        for k in range(1, peers):
            hand(source, target, owner, k, sent, received).start()

        @pl.when(boss)
        def _():
            mine = pl.ds(pl.multiple_of(me * kept, kept), kept)
            target[owner, block] = source[owner, mine, :]

    def gathered(target, owner, received):
        def some(amount):
            part = target.at[owner, pl.ds(0, amount)]
            pltpu.make_async_copy(part, part, received.at[owner]).wait()

        pl.when(boss)(lambda: some(peers - 1))
        pl.when(other)(lambda: some(peers))
        total = target[owner, 0].astype(jnp.float32)
        for k in range(1, peers):
            total = total + target[owner, k].astype(jnp.float32)
        return total

    def handed(target, sent):
        def some(amount):
            part = target.at[:, pl.ds(0, amount)]
            pltpu.make_async_copy(part, part, sent).wait()

        pl.when(boss)(lambda: some(peers - 1))
        pl.when(other)(lambda: some(peers))

    def project(owner):
        if lent:

            @pl.when(inner)
            def _():
                partial[owner] = (through(0, hidden[0], owner) + through(1, hidden[1], owner)).astype(
                    jnp.bfloat16
                )

            @pl.when(end)
            def _():
                partial[owner] = through(0, hidden[0], owner).astype(jnp.bfloat16)

        else:
            partial[owner] = through(0, hidden[0], owner).astype(jnp.bfloat16)
        hand_out(partial, landed, owner, sum_send, sum_recv)

    def guest_project(owner):
        @pl.when(helper)
        def _():
            guest_partial[owner] = through(1, guest_hidden, owner).astype(jnp.bfloat16)
            hand_out(guest_partial, guest_landed, owner, guest_sum_send, guest_sum_recv)

    def back(owner):
        return pltpu.make_async_remote_copy(
            src_ref=summed.at[owner],
            dst_ref=returned.at[owner],
            send_sem=back_send.at[owner],
            recv_sem=back_recv.at[owner],
            device_id={"fs": mate},
            device_id_type=MESH,
        )

    def give_back(owner):
        @pl.when(helper)
        def _():
            summed[owner] = gathered(guest_landed, owner, guest_sum_recv).astype(jnp.bfloat16)
            back(owner).start()

    for i, vector in enumerate((norm_gain, down_scale)):
        gains[i : i + 1, :] = vector[...].reshape(1, width)

    @pl.when(boss)
    def _():
        for i, (taps, scale, bias) in enumerate(
            ((value_taps, value_scale, value_bias), (gate_taps, gate_scale, gate_bias))
        ):
            along[3 * i : 3 * i + 3, :] = taps[...] * scale[...].reshape(1, units)
            along[6 + i : 7 + i, :] = bias[...].reshape(1, units)
        cast_up(kinds - 1)

    sides = (here == 0).astype(jnp.int32) + (here == line - 1).astype(jnp.int32)
    pl.semaphore_wait(barrier, parts * peers - 1 + 2 - sides)
    if lent:
        pl.when(both(boss, end))(lambda: lend().start())
    pl.when(boss)(lambda: swap().start())
    pieces_up(kinds - 1, lambda which: own_line(which, start))

    @pl.when(boss)
    def _():
        vectors().start()

    pieces_up(kinds - 1, lambda which: own_across(which, start))
    if lent:
        pl.when(boss)(lambda: cast_up(0))
        pieces_up(0, lambda which: own_line(which, start, True))
        pieces_up(0, lambda which: own_across(which, start))

    @pl.when(boss)
    def _():
        for kind in range(kinds):
            cast_down(kind)

    for kind in reversed(range(kinds)):
        pieces_down(kind, lambda which: own_line(which, start, True))
        pieces_down(kind, lambda which: own_across(which, start))

    if lent:
        pl.when(both(boss, helper))(relay)
    pl.when(boss)(lambda: normalize(tokens, normed))

    if lent:
        for i in range(1, line):
            pieces_up(1, lambda which: arrive(which, owner_at(i)))
            if i == 1:
                pieces_up(0, lambda which: own_line(which, start, False))

    @pl.when(other)
    def _():
        vectors().wait_recv()
        swap().wait_recv()
        normalize(raw, normed)

    if lent:
        pieces_up(1, at_home)

        @pl.when(inner)
        def _():
            groups(1, lambda name, q: up(1, name, q, normed, hidden[1]))

        pl.when(both(other, helper))(relay)

    def nearer(name, q):
        for r in range(CUT):
            at_home(piece(name, 0, q, r))
        for i in range(1, line - 1):
            for r in range(CUT):
                arrive(piece(name, 0, q, r), owner_at(i))

    groups(0, nearer)
    for kind in reversed(range(kinds)):
        pieces_down(kind, lambda which: own_line(which, start, False))

    if lent:

        @pl.when(helper)
        def _():
            welcome()
            groups(1, lambda name, q: up(1, name, q, guest_normed, guest_hidden))

    last = owner_at(line - 1)

    def farthest(name, q):
        for r in range(CUT):
            arrive(piece(name, 0, q, r), last)
        up(0, name, q, normed, hidden[0])

    groups(0, farthest)

    def finish_line(i, carry):
        owner = owner_at(i)
        for kind in reversed(range(kinds)):

            @pl.when(i == 0)
            def _():
                pieces_down(kind, at_home)

            @pl.when(i > 0)
            def _():
                pieces_down(kind, lambda which: arrive(which, owner))

            if kind:
                guest_project(owner)
        project(owner)
        if lent:
            pl.when(i > 0)(lambda: give_back(owner_at(i - 1)))
        return carry

    lax.fori_loop(0, line, finish_line, 0)
    if lent:
        give_back(last)

    def sum_up(i, carry):
        owner = owner_at(i)
        columns = pl.ds(pl.multiple_of(owner * held, held), held)
        total = gathered(landed, owner, sum_recv)

        def keep(amount):
            out[:, columns] = (amount * gains[1:2, columns]).astype(jnp.bfloat16)

        if lent:

            @pl.when(end)
            def _():
                back(owner).wait_recv()
                keep(total + returned[owner].astype(jnp.float32))

            pl.when(inner)(lambda: keep(total))
        else:
            keep(total)
        return carry

    lax.fori_loop(0, line, sum_up, 0)

    handed(landed, sum_send)

    @pl.when(boss)
    def _():
        swap().wait_send()
        vectors().wait_send()

    if lent:
        pl.when(both(boss, end))(lambda: lend().wait_send())

        @pl.when(helper)
        def _():
            pl.when(boss)(lambda: pass_across().wait_send())
            for k in range(1, pairs):
                pass_on(k).wait_send()
            handed(guest_landed, guest_sum_send)
            for owner in range(line):
                back(owner).wait_send()

    for kind in range(kinds):
        for visit in (pieces_up, pieces_down):
            visit(kind, lambda which: own_line(which, left))
            visit(kind, lambda which: own_across(which, left))
            for i in range(1, line):
                visit(kind, lambda which: onward(which, owner_at(i), left, False))


def solution(mesh):
    parts, line, peers = mesh.shape["grp"], mesh.shape["fs"], mesh.shape["tp"]

    def local(*arrays):
        rows, width = arrays[0].shape
        held, units = arrays[2].shape
        kept = rows // peers
        pairs = peers // parts
        lent = units * 5 // 11 // 128 * 128 if line >= 4 and peers > 1 else 0
        half, full = jnp.bfloat16, jnp.float32
        spans = (units - lent, lent) if lent else (units,)
        dma = pltpu.SemaphoreType.DMA
        scratch = [
            pltpu.VMEM((span // WIDE, 2, width, WIDE), half) for span in spans if span // WIDE
        ]
        scratch += [pltpu.VMEM((2, width, span % WIDE), half) for span in spans if span % WIDE]
        scratch += [pltpu.VMEM((width, span), half) for span in spans]
        scratch += [pltpu.VMEM((rows, span), half) for span in spans]
        pieces = sum((pl.cdiv(span, WIDE) + 1) * CUT for span in spans)
        scratch += [
            pltpu.VMEM((rows, width), half),
            pltpu.VMEM((rows, width), half),
            pltpu.VMEM((8, units), full),
            pltpu.VMEM((2, width), full),
            pltpu.VMEM((line, rows, held), half),
            pltpu.VMEM((line, peers, kept, held), half),
            dma((pieces, line, 3)),
            dma((pieces, line)),
            dma((2,)),
            dma((2,)),
            dma,
            dma((line,)),
        ]
        if lent:
            scratch += [
                pltpu.VMEM((rows, width), half),
                pltpu.VMEM((rows, width), half),
                pltpu.VMEM((rows, lent), half),
                pltpu.VMEM((line, rows, held), half),
                pltpu.VMEM((line, peers, kept, held), half),
                pltpu.VMEM((line, kept, held), half),
                pltpu.VMEM((line, kept, held), half),
                dma((pairs + 1,)),
                dma((pairs,)),
                dma,
                dma((line,)),
                dma((line,)),
                dma((line,)),
            ]
        return pl.pallas_call(
            functools.partial(kernel, parts, line, peers, lent),
            out_shape=jax.ShapeDtypeStruct((kept, width), half),
            in_specs=[pl.BlockSpec(memory_space=pltpu.VMEM)] * 12,
            out_specs=pl.BlockSpec(memory_space=pltpu.VMEM),
            scratch_shapes=scratch,
            compiler_params=pltpu.CompilerParams(
                collective_id=0, has_side_effects=True, vmem_limit_bytes=62 * 1024 * 1024
            ),
        )(*arrays)

    return jax.shard_map(
        local,
        mesh=mesh,
        in_specs=(
            P(("grp", "fs"), None),
            P(),
            P("fs", "tp"),
            P("fs", "tp"),
            P("fs", "tp"),
            P("tp"),
            P("tp"),
            P(),
            P(None, "tp"),
            P(None, "tp"),
            P("tp"),
            P("tp"),
        ),
        out_specs=P(("grp", "fs", "tp"), None),
        check_vma=False,
    )
```

```python
import functools

import jax
import jax.numpy as jnp
from jax import lax
from jax.experimental import pallas as pl
from jax.experimental.pallas import tpu as pltpu
from jax.sharding import PartitionSpec as P

MESH = pl.DeviceIdType.MESH
WIDE = 256
CUT = 2


def kernel(
    parts,
    line,
    peers,
    lent,
    slices,
    tokens,
    norm_gain,
    value_weight,
    gate_weight,
    down_weight,
    value_scale,
    gate_scale,
    down_scale,
    value_taps,
    gate_taps,
    value_bias,
    gate_bias,
    out,
    *scratch,
):
    group, here, me = lax.axis_index("grp"), lax.axis_index("fs"), lax.axis_index("tp")
    scratch = list(scratch)
    take = lambda count: [scratch.pop(0) for _ in range(count)]
    kinds = 2 if lent else 1
    rows, width = tokens.shape
    held, units = value_weight.shape
    thin = held // slices
    kept = rows // peers
    pairs = peers // parts
    base = (0, units - lent)
    span = (units - lent, lent)
    many = [span[k] // WIDE for k in range(kinds)]
    left_over = [span[k] % WIDE for k in range(kinds)]
    wide = [take(1)[0] if many[k] else None for k in range(kinds)]
    rest = [take(1)[0] if left_over[k] else None for k in range(kinds)]
    down = take(kinds)
    hidden = take(kinds)
    value_load, gate_load, down_load, token_load = take(4)
    raw, normed, along, gains, partial, landed = take(6)
    send_sem, recv_sem, load_sem, token_sem, along_sem, sum_send, sum_recv = take(7)
    if lent:
        guest, guest_normed, guest_hidden, guest_partial, guest_landed, summed, returned = take(7)
        guest_send, guest_recv, guest_sum_send, guest_sum_recv, back_send, back_recv = take(6)

    pair = lax.div(me, parts)
    core = lax.rem(me, parts)
    boss = core == group
    other = jnp.logical_not(boss)
    block = pair * parts + group
    sibling = pair * parts + lax.rem(core + 1, parts)
    end = jnp.logical_or(here == 0, here == line - 1)
    inner = jnp.logical_not(end)
    helper = jnp.logical_and(inner, jnp.logical_or(here == 1, here == line - 2))
    mate = jnp.where(end, jnp.where(here == 0, 1, line - 2), jnp.where(here == 1, 0, line - 1))
    both = jnp.logical_and

    barrier = pltpu.get_barrier_semaphore()

    def greet(target):
        pl.semaphore_signal(barrier, inc=1, device_id=target, device_id_type=MESH)

    pl.when(here > 0)(lambda: greet({"fs": here - 1}))
    pl.when(here < line - 1)(lambda: greet({"fs": here + 1}))
    for j in range(parts):
        for k in range(peers):
            if j or k:
                greet({"grp": lax.rem(group + j, parts), "tp": lax.rem(me + k, peers)})

    def owner_at(i):
        near = jnp.where(here < line // 2, here, line - 1 - here)
        turned = jnp.where(i % 2 == 1, near - (i + 1) // 2, near + i // 2)
        first = jnp.where(i > 2 * near, i, turned)
        return jnp.where(here < line // 2, first, line - 1 - first)

    def slice_at(j):
        return owner_at(j // slices) * slices + j % slices

    numbers, stores = {}, {}
    count = 0
    for k in range(kinds):
        for name, amount in (("wide", many[k] * CUT), ("rest", CUT), ("down", slices)):
            stores[name, k] = len(stores)
            numbers[name, k] = count
            count += amount if name != "rest" or left_over[k] else 0

    def store_rows(name, kind, taken):
        if name == "wide":
            return wide[kind].at[:, :, taken, :]
        if name == "rest":
            return rest[kind].at[:, taken, :]
        return down[kind].at[taken, :]

    def piece(name, kind, q, r):
        cut = slices if name == "down" else CUT

        def ref(owner):
            part = held // cut
            taken = pl.ds(pl.multiple_of(owner * held + r * part, part), part)
            return wide[kind].at[q, :, taken, :] if name == "wide" else store_rows(name, kind, taken)

        return numbers[name, kind] + q * CUT + r, kind, ref, stores[name, kind]

    def groups(kind, body):
        if many[kind]:

            def one(q, carry):
                body("wide", q)
                return carry

            lax.fori_loop(0, many[kind], one, 0)
        if left_over[kind]:
            body("rest", 0)

    def copy(which, owner, direction):
        number, kind, ref, store = which
        if direction is None:
            target, lane = {"tp": sibling}, 2
        else:
            target = {"fs": lax.clamp(0, here + direction, line - 1)}
            lane = jnp.where(direction > 0, 0, 1)
        return pltpu.make_async_remote_copy(
            src_ref=ref(owner),
            dst_ref=ref(owner),
            send_sem=send_sem.at[store, lane],
            recv_sem=recv_sem.at[number, owner],
            device_id=target,
            device_id_type=MESH,
        )

    def used(kind):
        return inner if kind else here >= 0

    def further(kind, direction):
        there = here + direction
        return both(there >= kind, there <= line - 1 - kind)

    def toward_end(direction):
        there = here + direction
        return jnp.logical_or(end, jnp.logical_or(there == 0, there == line - 1))

    def own_line(which, early=None):
        for direction in (1, -1):
            go = both(boss, further(which[1], direction))
            if early is True:
                go = both(go, toward_end(direction))
            elif early is False:
                go = both(go, jnp.logical_not(toward_end(direction)))
            pl.when(go)(lambda: copy(which, here, direction).start())

    def own_across(which):
        pl.when(both(boss, used(which[1])))(lambda: copy(which, here, None).start())

    def arrive(which, owner):
        direction = jnp.where(owner < here, 1, -1)

        @pl.when(used(which[1]))
        def _():
            copy(which, owner, None).wait_recv()

            @pl.when(boss)
            def _():
                pl.when(further(which[1], direction))(lambda: copy(which, owner, direction).start())
                copy(which, owner, None).start()

    def at_home(which):
        pl.when(both(other, used(which[1])))(lambda: copy(which, here, None).wait_recv())

    def pieces_up(kind, body):
        def group_body(name, q):
            for r in range(CUT):
                body(piece(name, kind, q, r))

        groups(kind, group_body)

    def pieces_down(kind, body):
        for r in range(slices):
            body(piece("down", kind, 0, r))

    def cast_rows(source, columns, store):
        step = min(held, 64)

        def body(i, carry):
            taken = pl.ds(pl.multiple_of(i * step, step), step)
            target = pl.ds(pl.multiple_of(here * held + i * step, step), step)
            store(target, source[taken, columns].astype(jnp.bfloat16))
            return carry

        lax.fori_loop(0, held // step, body, 0)

    def load(number):
        if number < 2 * kinds:
            kind = kinds - 1 - number // 2
            columns = pl.ds(base[kind], span[kind])
            source, target = ((value_weight, value_load), (gate_weight, gate_load))[number % 2]
            source, target = source.at[:, columns], target.at[:, columns]
        elif number == 2 * kinds:
            source, target = tokens, token_load
        else:
            source, target = down_weight, down_load
        return pltpu.make_async_copy(source, target, load_sem.at[number])

    def loaded(kind):
        for m in range(2):
            load(2 * (kinds - 1 - kind) + m).wait()

    def cast_up(kind, begin, stop):
        for m, source in enumerate((value_load, gate_load)):
            for q in range(begin, stop):
                first = base[kind] + q * WIDE

                def store(target, values):
                    if q < many[kind]:
                        wide[kind][q, m, target, :] = values
                    else:
                        rest[kind][m, target, :] = values

                cast_rows(source, slice(first, min(first + WIDE, base[kind] + span[kind])), store)

    def cast_down(kind):
        def store(target, values):
            down[kind][target, :] = values

        cast_rows(down_load, slice(base[kind], base[kind] + span[kind]), store)

    def normalize(source, target):
        step = min(rows, 64)

        def body(i, carry):
            taken = pl.ds(pl.multiple_of(i * step, step), step)
            floated = source[taken, :].astype(jnp.float32)
            mean = jnp.mean(floated * floated, axis=-1, keepdims=True)
            target[taken, :] = (floated * lax.rsqrt(mean + 1e-06) * gains[0:1, :]).astype(
                jnp.bfloat16
            )
            return carry

        lax.fori_loop(0, rows // step, body, 0)

    def swap(part):
        taken = pl.ds(part * (rows // 2), rows // 2)
        return pltpu.make_async_remote_copy(
            src_ref=token_load.at[taken, :],
            dst_ref=raw.at[taken, :],
            send_sem=token_sem.at[part],
            recv_sem=token_sem.at[2 + part],
            device_id={"grp": lax.rem(group + 1, parts)},
            device_id_type=MESH,
        )

    def vectors():
        return pltpu.make_async_remote_copy(
            src_ref=along,
            dst_ref=along,
            send_sem=along_sem.at[0],
            recv_sem=along_sem.at[1],
            device_id={"tp": sibling},
            device_id_type=MESH,
        )

    share = rows // pairs

    def portion(ref):
        return ref.at[pl.ds(pl.multiple_of(pair * share, share), share), :]

    def guest_copy(source, slot, target):
        return pltpu.make_async_remote_copy(
            src_ref=portion(source),
            dst_ref=portion(guest),
            send_sem=guest_send.at[slot],
            recv_sem=guest_recv.at[pair],
            device_id=target,
            device_id_type=MESH,
        )

    def lend():
        return guest_copy(token_load, pairs, {"fs": mate})

    def pass_on(k):
        return guest_copy(guest, k, {"tp": lax.rem(me + k * parts, peers)})

    def pass_across():
        return guest_copy(guest, 0, {"grp": lax.rem(group + 1, parts)})

    def relay():
        lend().wait_recv()
        pl.when(boss)(lambda: pass_across().start())
        pl.when(boss)(lambda: swap(1).start())
        for k in range(1, pairs):
            pass_on(k).start()

    def welcome():
        for k in range(1, pairs):
            from_pair = lax.rem(pair + k, pairs)
            landed_share = guest.at[pl.ds(pl.multiple_of(from_pair * share, share), share), :]
            pltpu.make_async_copy(landed_share, landed_share, guest_recv.at[from_pair]).wait()
        normalize(guest, guest_normed)

    def causal(weight, tap, bias, source, outer):
        up = jnp.dot(source[...], weight[...], preferred_element_type=jnp.float32)
        position = lax.broadcasted_iota(jnp.int32, up.shape, 0)
        one = jnp.where(position >= 1, pltpu.roll(up, 1, axis=0), 0.0)
        two = jnp.where(position >= 2, pltpu.roll(up, 2, axis=0), 0.0)
        return (
            along[tap : tap + 1, outer] * two
            + along[tap + 1 : tap + 2, outer] * one
            + along[tap + 2 : tap + 3, outer] * up
            + along[bias : bias + 1, outer]
        )

    def up(kind, name, q, source, keep):
        weights = wide[kind].at[q] if name == "wide" else rest[kind]
        extent = WIDE if name == "wide" else left_over[kind]
        first = q * WIDE if name == "wide" else many[kind] * WIDE
        if name == "wide":
            first = pl.multiple_of(first, WIDE)
            outer = pl.ds(pl.multiple_of(base[kind] + first, 128), extent)
        else:
            outer = pl.ds(base[kind] + first, extent)
        value = causal(weights.at[0], 0, 6, source, outer)
        gate = causal(weights.at[1], 3, 7, source, outer)
        keep[:, pl.ds(first, extent)] = (gate / (1.0 + jnp.exp(-gate)) * value).astype(jnp.bfloat16)

    def through(kind, activations, owner):
        shard = down[kind][pl.ds(pl.multiple_of(owner * thin, thin), thin), :]
        return lax.dot_general(
            activations[...], shard, (((1,), (1,)), ((), ())), preferred_element_type=jnp.float32
        )

    def hand(source, target, owner, k, sent, received):
        peer = lax.rem(me + k, peers)
        return pltpu.make_async_remote_copy(
            src_ref=source.at[owner, pl.ds(pl.multiple_of(peer * kept, kept), kept), :],
            dst_ref=target.at[owner, block],
            send_sem=sent,
            recv_sem=received.at[owner],
            device_id={"grp": core, "tp": peer},
            device_id_type=MESH,
        )

    def hand_out(source, target, owner, sent, received):
        pl.when(other)(lambda: hand(source, target, owner, 0, sent, received).start())
        for k in range(1, peers):
            hand(source, target, owner, k, sent, received).start()

        @pl.when(boss)
        def _():
            mine = pl.ds(pl.multiple_of(me * kept, kept), kept)
            target[owner, block] = source[owner, mine, :]

    def gathered(target, owner, received):
        def some(amount):
            part = target.at[owner, pl.ds(0, amount)]
            pltpu.make_async_copy(part, part, received.at[owner]).wait()

        pl.when(boss)(lambda: some(peers - 1))
        pl.when(other)(lambda: some(peers))
        total = target[owner, 0].astype(jnp.float32)
        for k in range(1, peers):
            total = total + target[owner, k].astype(jnp.float32)
        return total

    def handed(target, sent):
        def some(amount):
            part = target.at[:, pl.ds(0, amount)]
            pltpu.make_async_copy(part, part, sent).wait()

        pl.when(boss)(lambda: some(peers - 1))
        pl.when(other)(lambda: some(peers))

    def project(owner):
        if lent:

            @pl.when(inner)
            def _():
                partial[owner] = (through(0, hidden[0], owner) + through(1, hidden[1], owner)).astype(
                    jnp.bfloat16
                )

            @pl.when(end)
            def _():
                partial[owner] = through(0, hidden[0], owner).astype(jnp.bfloat16)

        else:
            partial[owner] = through(0, hidden[0], owner).astype(jnp.bfloat16)
        hand_out(partial, landed, owner, sum_send, sum_recv)

    def guest_project(owner):
        @pl.when(helper)
        def _():
            guest_partial[owner] = through(1, guest_hidden, owner).astype(jnp.bfloat16)
            hand_out(guest_partial, guest_landed, owner, guest_sum_send, guest_sum_recv)

    def back(owner):
        return pltpu.make_async_remote_copy(
            src_ref=summed.at[owner],
            dst_ref=returned.at[owner],
            send_sem=back_send,
            recv_sem=back_recv.at[owner],
            device_id={"fs": mate},
            device_id_type=MESH,
        )

    def give_back(owner):
        @pl.when(helper)
        def _():
            summed[owner] = gathered(guest_landed, owner, guest_sum_recv).astype(jnp.bfloat16)
            back(owner).start()

    scope = jax.named_scope

    @pl.when(boss)
    def _():
        for number in (*range(2), 2 * kinds, 2 * kinds + 1, *range(2, 2 * kinds)):
            load(number).start()

    with scope("vectors"):
        for i, vector in enumerate((norm_gain, down_scale)):
            gains[i : i + 1, :] = vector[...].reshape(1, width)

        @pl.when(boss)
        def _():
            for i, (taps, scale, bias) in enumerate(
                ((value_taps, value_scale, value_bias), (gate_taps, gate_scale, gate_bias))
            ):
                along[3 * i : 3 * i + 3, :] = taps[...] * scale[...].reshape(1, units)
                along[6 + i : 7 + i, :] = bias[...].reshape(1, units)

    amounts = [many[k] + (1 if left_over[k] else 0) for k in range(kinds)]
    first = ("wide", 0) if many[0] else ("rest", 0)

    def others(body):
        if many[0] > 1:

            def one(q, carry):
                body("wide", q)
                return carry

            lax.fori_loop(1, many[0], one, 0)
        if left_over[0] and many[0]:
            body("rest", 0)

    def each(name, q, body):
        for r in range(CUT):
            body(piece(name, 0, q, r))

    with scope("cast_first"):

        @pl.when(boss)
        def _():
            loaded(kinds - 1)
            cast_up(kinds - 1, 0, amounts[-1])

    with scope("barrier"):
        sides = (here == 0).astype(jnp.int32) + (here == line - 1).astype(jnp.int32)
        pl.semaphore_wait(barrier, parts * peers - 1 + 2 - sides)
    with scope("send_first"):
        if lent:

            @pl.when(both(boss, end))
            def _():
                load(2 * kinds).wait()
                lend().start()

        pieces_up(kinds - 1, own_line)

        @pl.when(boss)
        def _():
            pl.when(inner if lent else boss)(lambda: load(2 * kinds).wait())
            swap(0).start()
            pl.when(jnp.logical_not(helper) if lent else boss)(lambda: swap(1).start())
            vectors().start()

        pieces_up(kinds - 1, own_across)
    with scope("cast_rest"):
        if lent:

            @pl.when(boss)
            def _():
                loaded(0)
                cast_up(0, 0, 1)

            each(*first, own_line)
        pl.when(boss)(lambda: load(2 * kinds + 1).wait())
        if lent:
            pl.when(boss)(lambda: cast_down(1))
            pieces_down(1, lambda which: own_line(which, True))
            pl.when(boss)(lambda: cast_up(0, 1, amounts[0]))
            others(lambda name, q: each(name, q, lambda which: own_line(which, True)))
            pieces_up(0, own_across)
        pl.when(boss)(lambda: cast_down(0))
        pieces_down(0, lambda which: own_line(which, True))
        for kind in reversed(range(kinds)):
            pieces_down(kind, own_across)

    with scope("normalize"):
        pl.when(boss)(lambda: normalize(token_load, normed))

    last = owner_at(line - 1)

    def nearer(name, q):
        with scope("a_near"):
            each(name, q, at_home)
            for i in reversed(range(1, line - 1)):
                each(name, q, lambda which: arrive(which, owner_at(i)))

    def farthest(name, q):
        with scope("a_far"):
            each(name, q, lambda which: arrive(which, last))

    if lent:
        with scope("relay"):
            pl.when(helper)(relay)

        def b_near(which):
            for i in range(1, line - 1):
                arrive(which, owner_at(i))

        with scope("b_near"):
            pieces_up(1, b_near)

    nearer(*first)
    if lent:
        others(lambda name, q: each(name, q, lambda which: own_line(which, False)))

    with scope("other_tokens"):

        @pl.when(other)
        def _():
            vectors().wait_recv()
            swap(0).wait_recv()
            swap(1).wait_recv()
            normalize(raw, normed)

    if lent:
        with scope("b_far"):
            pieces_up(1, at_home)
            pieces_up(1, lambda which: arrive(which, last))
        with scope("b_own"):

            @pl.when(inner)
            def _():
                groups(1, lambda name, q: up(1, name, q, normed, hidden[1]))
    farthest(*first)
    if lent:
        with scope("guest_wait"):
            pl.when(helper)(welcome)
        with scope("b_guest"):

            @pl.when(helper)
            def _():
                groups(1, lambda name, q: up(1, name, q, guest_normed, guest_hidden))

    def guest_early():
        with scope("guest_early"):
            pieces_down(1, at_home)
            pieces_down(1, lambda which: arrive(which, owner_at(1)))

            def early(j, carry):
                guest_project(slice_at(j))
                return carry

            lax.fori_loop(0, 2 * slices, early, 0)

    others(nearer)
    if lent:
        guest_early()

    def own_down(begin, stop):
        for r in range(begin, stop):
            for kind in range(kinds):
                own_line(piece("down", kind, 0, r), False)

    def own_up(name, q):
        final = q == many[0] - 1 if not left_over[0] else here < (line if name == "rest" else 0)
        pl.when(final)(lambda: own_down(0, 1))
        if name == "wide" or many[0]:
            pl.when(jnp.logical_or(name == "rest", q > 0))(lambda: farthest(name, q))
        pl.when(final)(lambda: own_down(1, slices))
        with scope("a_own"):
            up(0, name, q, normed, hidden[0])

    groups(0, own_up)

    def collect(at):
        columns = pl.ds(pl.multiple_of(at * thin, thin), thin)
        total = gathered(landed, at, sum_recv)

        def keep(amount):
            out[:, columns] = (amount * gains[1:2, columns]).astype(jnp.bfloat16)

        if lent:

            @pl.when(end)
            def _():
                back(at).wait_recv()
                keep(total + returned[at].astype(jnp.float32))

            pl.when(inner)(lambda: keep(total))
        else:
            keep(total)

    total_slices = line * slices
    lag = min(2 * slices, total_slices)
    late = max(slices - 1, 1)

    def finish_line(j, carry):
        i, r = j // slices, j % slices
        owner = owner_at(i)
        for kind in range(kinds):
            which = piece("down", kind, 0, r)
            with scope(f"c_arrive#k={kind}"):
                if kind:
                    pl.when(i > 1)(lambda: arrive(which, owner))
                else:
                    pl.when(i == 0)(lambda: at_home(which))
                    pl.when(i > 0)(lambda: arrive(which, owner))
        if lent:
            with scope("c_guest"):
                pl.when(i > 1)(lambda: guest_project(owner * slices + r))
            with scope("give_back"):
                pl.when(i < 2)(lambda: give_back(slice_at(j)))
        with scope("c_own"):
            project(owner * slices + r)
        if lent:
            with scope("give_back"):
                pl.when(j >= 2 * slices + late)(lambda: give_back(slice_at(j - late)))
        with scope("collect"):
            pl.when(j >= lag)(lambda: collect(slice_at(j - lag)))
        return carry

    lax.fori_loop(0, total_slices, finish_line, 0)

    if lent:


        def give_rest(j, carry):
            with scope("give_rest"):
                give_back(slice_at(j))
            return carry

        lax.fori_loop(total_slices - late, total_slices, give_rest, 0)

    def rest_of_line(j, carry):
        with scope("collect_rest"):
            collect(slice_at(j))
        return carry

    lax.fori_loop(total_slices - lag, total_slices, rest_of_line, 0)

    def departed(name, kind, amount, lane):
        part = store_rows(name, kind, pl.ds(0, amount * held))
        pltpu.make_async_copy(part, part, send_sem.at[stores[name, kind], lane]).wait()

    with scope("left"):
        handed(landed, sum_send)

        @pl.when(boss)
        def _():
            swap(0).wait_send()
            swap(1).wait_send()
            vectors().wait_send()
            for kind in range(kinds):
                for name, there in (("wide", many[kind]), ("rest", left_over[kind]), ("down", 1)):
                    if there:
                        for lane, direction in ((0, 1), (1, -1)):
                            amount = here + 1 if direction > 0 else line - here
                            for some in range(1, line):
                                pl.when(both(amount == some, further(kind, direction)))(
                                    lambda: departed(name, kind, some, lane)
                                )
                        pl.when(used(kind))(lambda: departed(name, kind, line, 2))

        if lent:
            pl.when(both(boss, end))(lambda: lend().wait_send())

            @pl.when(helper)
            def _():
                pl.when(boss)(lambda: pass_across().wait_send())
                for k in range(1, pairs):
                    pass_on(k).wait_send()
                handed(guest_landed, guest_sum_send)
                pltpu.make_async_copy(summed, summed, back_send).wait()


def solution(mesh):
    parts, line, peers = mesh.shape["grp"], mesh.shape["fs"], mesh.shape["tp"]

    def local(*arrays):
        rows, width = arrays[0].shape
        held, units = arrays[2].shape
        kept = rows // peers
        pairs = peers // parts
        lent = units * 6 // 11 // 128 * 128 if line >= 4 and peers > 1 else 0
        slices = 4 if held % 512 == 0 else 1
        thin = held // slices
        half, full = jnp.bfloat16, jnp.float32
        spans = (units - lent, lent) if lent else (units,)
        dma = pltpu.SemaphoreType.DMA
        scratch = [
            pltpu.VMEM((span // WIDE, 2, width, WIDE), half) for span in spans if span // WIDE
        ]
        scratch += [pltpu.VMEM((2, width, span % WIDE), half) for span in spans if span % WIDE]
        scratch += [pltpu.VMEM((width, span), half) for span in spans]
        scratch += [pltpu.VMEM((rows, span), half) for span in spans]
        pieces = sum(pl.cdiv(span, WIDE) * CUT + slices for span in spans)
        scratch += [
            pltpu.VMEM((held, units), full),
            pltpu.VMEM((held, units), full),
            pltpu.VMEM((held, units), full),
            pltpu.VMEM((rows, width), half),
            pltpu.VMEM((rows, width), half),
            pltpu.VMEM((rows, width), half),
            pltpu.VMEM((8, units), full),
            pltpu.VMEM((2, width), full),
            pltpu.VMEM((line * slices, rows, thin), half),
            pltpu.VMEM((line * slices, peers, kept, thin), half),
            dma((3 * len(spans), 3)),
            dma((pieces, line)),
            dma((2 * len(spans) + 2,)),
            dma((4,)),
            dma((2,)),
            dma,
            dma((line * slices,)),
        ]
        if lent:
            scratch += [
                pltpu.VMEM((rows, width), half),
                pltpu.VMEM((rows, width), half),
                pltpu.VMEM((rows, lent), half),
                pltpu.VMEM((line * slices, rows, thin), half),
                pltpu.VMEM((line * slices, peers, kept, thin), half),
                pltpu.VMEM((line * slices, kept, thin), half),
                pltpu.VMEM((line * slices, kept, thin), half),
                dma((pairs + 1,)),
                dma((pairs,)),
                dma,
                dma((line * slices,)),
                dma,
                dma((line * slices,)),
            ]
        return pl.pallas_call(
            functools.partial(kernel, parts, line, peers, lent, slices),
            out_shape=jax.ShapeDtypeStruct((kept, width), half),
            in_specs=[
                pl.BlockSpec(memory_space=pl.ANY if i in (0, 2, 3, 4) else pltpu.VMEM)
                for i in range(12)
            ],
            out_specs=pl.BlockSpec(memory_space=pltpu.VMEM),
            scratch_shapes=scratch,
            compiler_params=pltpu.CompilerParams(
                collective_id=0, has_side_effects=True, vmem_limit_bytes=62 * 1024 * 1024
            ),
        )(*arrays)

    return jax.shard_map(
        local,
        mesh=mesh,
        in_specs=(
            P(("grp", "fs"), None),
            P(),
            P("fs", "tp"),
            P("fs", "tp"),
            P("fs", "tp"),
            P("tp"),
            P("tp"),
            P(),
            P(None, "tp"),
            P(None, "tp"),
            P("tp"),
            P("tp"),
        ),
        out_specs=P(("grp", "fs", "tp"), None),
        check_vma=False,
    )
```

```python
import functools

import jax
import jax.numpy as jnp
from jax import lax
from jax.experimental import pallas as pl
from jax.experimental.pallas import tpu as pltpu
from jax.sharding import PartitionSpec as P

MESH = pl.DeviceIdType.MESH
WIDE = 256
CUT = 2


def kernel(
    parts,
    line,
    peers,
    lent,
    slices,
    tokens,
    norm_gain,
    value_weight,
    gate_weight,
    down_weight,
    value_scale,
    gate_scale,
    down_scale,
    value_taps,
    gate_taps,
    value_bias,
    gate_bias,
    out,
    *scratch,
):
    group, here, me = lax.axis_index("grp"), lax.axis_index("fs"), lax.axis_index("tp")
    scratch = list(scratch)
    take = lambda count: [scratch.pop(0) for _ in range(count)]
    kinds = 2 if lent else 1
    rows, width = tokens.shape
    held, units = value_weight.shape
    thin = held // slices
    kept = rows // peers
    pairs = peers // parts
    base = (0, units - lent)
    span = (units - lent, lent)
    many = [span[k] // WIDE for k in range(kinds)]
    left_over = [span[k] % WIDE for k in range(kinds)]
    wide = [take(1)[0] if many[k] else None for k in range(kinds)]
    rest = [take(1)[0] if left_over[k] else None for k in range(kinds)]
    down = take(kinds)
    hidden = take(kinds)
    value_load, gate_load, down_load, token_load = take(4)
    raw, normed, along, gains, partial, landed, x_stage = take(7)
    send_sem, recv_sem, load_sem, token_sem, along_sem = take(5)
    sum_send, sum_recv, x_send, x_recv = take(4)
    if lent:
        guest, guest_normed, guest_hidden, guest_partial, guest_landed, y_stage = take(6)
        summed, returned, guest_send, guest_recv, back_send, back_recv = take(6)
        guest_sum_send, guest_direct, guest_sum_recv, y_send, y_recv = take(5)

    pair = lax.div(me, parts)
    core = lax.rem(me, parts)
    boss = core == group
    other = jnp.logical_not(boss)
    block = pair * parts + group
    sibling = pair * parts + lax.rem(core + 1, parts)
    end = jnp.logical_or(here == 0, here == line - 1)
    inner = jnp.logical_not(end)
    helper = jnp.logical_and(inner, jnp.logical_or(here == 1, here == line - 2))
    mate = jnp.where(end, jnp.where(here == 0, 1, line - 2), jnp.where(here == 1, 0, line - 1))
    both = jnp.logical_and

    barrier = pltpu.get_barrier_semaphore()

    def greet(target):
        pl.semaphore_signal(barrier, inc=1, device_id=target, device_id_type=MESH)

    pl.when(here > 0)(lambda: greet({"fs": here - 1}))
    pl.when(here < line - 1)(lambda: greet({"fs": here + 1}))
    for j in range(parts):
        for k in range(peers):
            if j or k:
                greet({"grp": lax.rem(group + j, parts), "tp": lax.rem(me + k, peers)})

    def owner_at(i):
        near = jnp.where(here < line // 2, here, line - 1 - here)
        turned = jnp.where(i % 2 == 1, near - (i + 1) // 2, near + i // 2)
        first = jnp.where(i > 2 * near, i, turned)
        return jnp.where(here < line // 2, first, line - 1 - first)

    def turn(p):
        if line != 4:
            return owner_at(p)
        return owner_at(jnp.where(p < 2, p, 5 - p))

    def slice_at(j):
        return turn(j // slices) * slices + j % slices

    numbers, stores = {}, {}
    count = 0
    for k in range(kinds):
        for name, amount in (("wide", many[k] * CUT), ("rest", CUT), ("down", slices)):
            stores[name, k] = len(stores)
            numbers[name, k] = count
            count += amount if name != "rest" or left_over[k] else 0

    def store_rows(name, kind, taken):
        if name == "wide":
            return wide[kind].at[:, :, taken, :]
        if name == "rest":
            return rest[kind].at[:, taken, :]
        return down[kind].at[taken, :]

    def piece(name, kind, q, r):
        cut = slices if name == "down" else CUT

        def ref(owner):
            part = held // cut
            taken = pl.ds(pl.multiple_of(owner * held + r * part, part), part)
            return wide[kind].at[q, :, taken, :] if name == "wide" else store_rows(name, kind, taken)

        return numbers[name, kind] + q * CUT + r, kind, ref, stores[name, kind]

    def groups(kind, body):
        if many[kind]:

            def one(q, carry):
                body("wide", q)
                return carry

            lax.fori_loop(0, many[kind], one, 0)
        if left_over[kind]:
            body("rest", 0)

    def copy(which, owner, direction):
        number, kind, ref, store = which
        if direction is None:
            target, lane = {"tp": sibling}, 2
        else:
            target = {"fs": lax.clamp(0, here + direction, line - 1)}
            lane = jnp.where(direction > 0, 0, 1)
        return pltpu.make_async_remote_copy(
            src_ref=ref(owner),
            dst_ref=ref(owner),
            send_sem=send_sem.at[store, lane],
            recv_sem=recv_sem.at[number, owner],
            device_id=target,
            device_id_type=MESH,
        )

    def used(kind):
        return inner if kind else here >= 0

    def further(kind, direction):
        there = here + direction
        return both(there >= kind, there <= line - 1 - kind)

    def toward_end(direction):
        there = here + direction
        return jnp.logical_or(end, jnp.logical_or(there == 0, there == line - 1))

    def own_line(which, early=None):
        for direction in (1, -1):
            go = both(boss, further(which[1], direction))
            if early is True:
                go = both(go, toward_end(direction))
            elif early is False:
                go = both(go, jnp.logical_not(toward_end(direction)))
            pl.when(go)(lambda: copy(which, here, direction).start())

    def own_across(which):
        pl.when(both(boss, used(which[1])))(lambda: copy(which, here, None).start())

    def arrive_here(which, owner):
        @pl.when(used(which[1]))
        def _():
            copy(which, owner, None).wait_recv()
            pl.when(boss)(lambda: copy(which, owner, None).start())

    def pass_along(which, owner):
        direction = jnp.where(owner < here, 1, -1)
        go = both(both(boss, used(which[1])), further(which[1], direction))
        pl.when(go)(lambda: copy(which, owner, direction).start())

    def arrive(which, owner):
        direction = jnp.where(owner < here, 1, -1)

        @pl.when(used(which[1]))
        def _():
            copy(which, owner, None).wait_recv()

            @pl.when(boss)
            def _():
                pl.when(further(which[1], direction))(lambda: copy(which, owner, direction).start())
                copy(which, owner, None).start()

    def at_home(which):
        pl.when(both(other, used(which[1])))(lambda: copy(which, here, None).wait_recv())

    def pieces_up(kind, body):
        def group_body(name, q):
            for r in range(CUT):
                body(piece(name, kind, q, r))

        groups(kind, group_body)

    def pieces_down(kind, body):
        for r in range(slices):
            body(piece("down", kind, 0, r))

    def cast_rows(source, columns, store):
        step = min(held, 64)

        def body(i, carry):
            taken = pl.ds(pl.multiple_of(i * step, step), step)
            target = pl.ds(pl.multiple_of(here * held + i * step, step), step)
            store(target, source[taken, columns].astype(jnp.bfloat16))
            return carry

        lax.fori_loop(0, held // step, body, 0)

    def load(number):
        if number < 2 * kinds:
            kind = kinds - 1 - number // 2
            columns = pl.ds(base[kind], span[kind])
            source, target = ((value_weight, value_load), (gate_weight, gate_load))[number % 2]
            source, target = source.at[:, columns], target.at[:, columns]
        elif number == 2 * kinds:
            source, target = tokens, token_load
        else:
            source, target = down_weight, down_load
        return pltpu.make_async_copy(source, target, load_sem.at[number])

    def loaded(kind):
        for m in range(2):
            load(2 * (kinds - 1 - kind) + m).wait()

    def cast_up(kind, begin, stop):
        for m, source in enumerate((value_load, gate_load)):
            for q in range(begin, stop):
                first = base[kind] + q * WIDE

                def store(target, values):
                    if q < many[kind]:
                        wide[kind][q, m, target, :] = values
                    else:
                        rest[kind][m, target, :] = values

                cast_rows(source, slice(first, min(first + WIDE, base[kind] + span[kind])), store)

    def cast_down(kind):
        def store(target, values):
            down[kind][target, :] = values

        cast_rows(down_load, slice(base[kind], base[kind] + span[kind]), store)

    def normalize(source, target):
        step = min(rows, 64)

        def body(i, carry):
            taken = pl.ds(pl.multiple_of(i * step, step), step)
            floated = source[taken, :].astype(jnp.float32)
            mean = jnp.mean(floated * floated, axis=-1, keepdims=True)
            target[taken, :] = (floated * lax.rsqrt(mean + 1e-06) * gains[0:1, :]).astype(
                jnp.bfloat16
            )
            return carry

        lax.fori_loop(0, rows // step, body, 0)

    def swap(part):
        taken = pl.ds(part * (rows // 2), rows // 2)
        return pltpu.make_async_remote_copy(
            src_ref=token_load.at[taken, :],
            dst_ref=raw.at[taken, :],
            send_sem=token_sem.at[part],
            recv_sem=token_sem.at[2 + part],
            device_id={"grp": lax.rem(group + 1, parts)},
            device_id_type=MESH,
        )

    def vectors():
        return pltpu.make_async_remote_copy(
            src_ref=along,
            dst_ref=along,
            send_sem=along_sem.at[0],
            recv_sem=along_sem.at[1],
            device_id={"tp": sibling},
            device_id_type=MESH,
        )

    share = rows // pairs

    def portion(ref):
        return ref.at[pl.ds(pl.multiple_of(pair * share, share), share), :]

    def guest_copy(source, slot, target):
        return pltpu.make_async_remote_copy(
            src_ref=portion(source),
            dst_ref=portion(guest),
            send_sem=guest_send.at[slot],
            recv_sem=guest_recv.at[pair],
            device_id=target,
            device_id_type=MESH,
        )

    def lend():
        return guest_copy(token_load, pairs, {"fs": mate})

    def pass_on(k):
        return guest_copy(guest, k, {"tp": lax.rem(me + k * parts, peers)})

    def pass_across():
        return guest_copy(guest, 0, {"grp": lax.rem(group + 1, parts)})

    def relay():
        lend().wait_recv()
        pl.when(boss)(lambda: pass_across().start())
        pl.when(boss)(lambda: swap(1).start())
        for k in range(1, pairs):
            pass_on(k).start()

    def welcome():
        for k in range(1, pairs):
            from_pair = lax.rem(pair + k, pairs)
            landed_share = guest.at[pl.ds(pl.multiple_of(from_pair * share, share), share), :]
            pltpu.make_async_copy(landed_share, landed_share, guest_recv.at[from_pair]).wait()
        normalize(guest, guest_normed)

    def causal(weight, tap, bias, source, outer):
        up = jnp.dot(source[...], weight[...], preferred_element_type=jnp.float32)
        position = lax.broadcasted_iota(jnp.int32, up.shape, 0)
        one = jnp.where(position >= 1, pltpu.roll(up, 1, axis=0), 0.0)
        two = jnp.where(position >= 2, pltpu.roll(up, 2, axis=0), 0.0)
        return (
            along[tap : tap + 1, outer] * two
            + along[tap + 1 : tap + 2, outer] * one
            + along[tap + 2 : tap + 3, outer] * up
            + along[bias : bias + 1, outer]
        )

    def up(kind, name, q, source, keep):
        weights = wide[kind].at[q] if name == "wide" else rest[kind]
        extent = WIDE if name == "wide" else left_over[kind]
        first = q * WIDE if name == "wide" else many[kind] * WIDE
        if name == "wide":
            first = pl.multiple_of(first, WIDE)
            outer = pl.ds(pl.multiple_of(base[kind] + first, 128), extent)
        else:
            outer = pl.ds(base[kind] + first, extent)
        value = causal(weights.at[0], 0, 6, source, outer)
        gate = causal(weights.at[1], 3, 7, source, outer)
        keep[:, pl.ds(first, extent)] = (gate / (1.0 + jnp.exp(-gate)) * value).astype(jnp.bfloat16)

    def through(kind, activations, owner):
        shard = down[kind][pl.ds(pl.multiple_of(owner * thin, thin), thin), :]
        return lax.dot_general(
            activations[...], shard, (((1,), (1,)), ((), ())), preferred_element_type=jnp.float32
        )

    def hand(source, target, at, slot, to_group, peer, sent, received):
        return pltpu.make_async_remote_copy(
            src_ref=source.at[at, pl.ds(pl.multiple_of(peer * kept, kept), kept), :],
            dst_ref=target.at[at, slot],
            send_sem=sent,
            recv_sem=received.at[at],
            device_id={"grp": to_group, "tp": peer},
            device_id_type=MESH,
        )

    mine = pl.ds(pl.multiple_of(me * kept, kept), kept)
    folded = (line - 1) * slices

    def direct(source, target, at, sent, received):
        for k in range(peers):
            peer = lax.rem(me + k, peers)
            copy_out = hand(source, target, at, block, core, peer, sent, received)
            pl.when(other if k == 0 else here >= 0)(lambda: copy_out.start())

        @pl.when(boss)
        def _():
            target[at, block] = source[at, mine, :]

    def across(at):
        return pltpu.make_async_remote_copy(
            src_ref=partial.at[at],
            dst_ref=x_stage.at[at],
            send_sem=x_send,
            recv_sem=x_recv.at[at],
            device_id={"grp": lax.rem(group + 1, parts)},
            device_id_type=MESH,
        )

    def fold(at):
        @pl.when(boss)
        def _():
            across(at).wait_recv()
            total = partial[at].astype(jnp.float32) + x_stage[at].astype(jnp.float32)
            partial[at] = total.astype(jnp.bfloat16)
            for k in range(1, peers):
                peer = lax.rem(me + k, peers)
                hand(partial, landed, at, pair, group, peer, sum_send, sum_recv).start()
            landed[at, pair] = partial[at, mine, :]

    pair_rows = parts * kept

    def beside(at, k):
        there = pl.multiple_of(lax.rem(pair + k, pairs) * pair_rows, pair_rows)
        return pltpu.make_async_remote_copy(
            src_ref=guest_partial.at[at, pl.ds(there, pair_rows), :],
            dst_ref=y_stage.at[at, k - 1],
            send_sem=y_send,
            recv_sem=y_recv.at[at],
            device_id={"tp": lax.rem(me + k * parts, peers)},
            device_id_type=MESH,
        )

    def guest_fold(at):
        ours = pl.ds(pl.multiple_of(pair * pair_rows, pair_rows), pair_rows)

        @pl.when(helper)
        def _():
            if pairs > 1:
                staged = y_stage.at[at, pl.ds(0, pairs - 1)]
                pltpu.make_async_copy(staged, staged, y_recv.at[at]).wait()
                total = guest_partial[at, ours, :].astype(jnp.float32)
                for k in range(1, pairs):
                    total = total + y_stage[at, k - 1].astype(jnp.float32)
                guest_partial[at, ours, :] = total.astype(jnp.bfloat16)
            for k in range(parts):
                peer = pair * parts + lax.rem(core + k, parts)
                copy_out = hand(
                    guest_partial, guest_landed, at, group, core, peer, guest_sum_send, guest_sum_recv
                )
                pl.when(other if k == 0 else here >= 0)(lambda: copy_out.start())

            @pl.when(boss)
            def _():
                guest_landed[at, group] = guest_partial[at, mine, :]

    def gathered(target, at, slots, received):
        def some(amount):
            if amount:
                part = target.at[at, pl.ds(0, amount)]
                pltpu.make_async_copy(part, part, received.at[at]).wait()

        pl.when(boss)(lambda: some(slots - 1))
        pl.when(other)(lambda: some(slots))
        total = target[at, 0].astype(jnp.float32)
        for k in range(1, slots):
            total = total + target[at, k].astype(jnp.float32)
        return total

    def handed(part, sent):
        pltpu.make_async_copy(part, part, sent).wait()

    def project(owner, is_last):
        if lent:

            @pl.when(inner)
            def _():
                partial[owner] = (through(0, hidden[0], owner) + through(1, hidden[1], owner)).astype(
                    jnp.bfloat16
                )

            @pl.when(end)
            def _():
                partial[owner] = through(0, hidden[0], owner).astype(jnp.bfloat16)

        else:
            partial[owner] = through(0, hidden[0], owner).astype(jnp.bfloat16)
        pl.when(is_last)(lambda: direct(partial, landed, owner, sum_send, sum_recv))
        pl.when(both(other, jnp.logical_not(is_last)))(lambda: across(owner).start())

    def guest_project(owner, is_last=None):
        @pl.when(helper)
        def _():
            guest_partial[owner] = through(1, guest_hidden, owner).astype(jnp.bfloat16)
            def besides():
                for k in range(1, pairs):
                    beside(owner, k).start()

            if is_last is None:
                besides()
            else:
                pl.when(jnp.logical_not(is_last))(besides)
                pl.when(is_last)(
                    lambda: direct(guest_partial, guest_landed, owner, guest_direct, guest_sum_recv)
                )

    def back(owner):
        return pltpu.make_async_remote_copy(
            src_ref=summed.at[owner],
            dst_ref=returned.at[owner],
            send_sem=back_send,
            recv_sem=back_recv.at[owner],
            device_id={"fs": mate},
            device_id_type=MESH,
        )

    def give_back(owner, slots):
        @pl.when(helper)
        def _():
            summed[owner] = gathered(guest_landed, owner, slots, guest_sum_recv).astype(jnp.bfloat16)
            back(owner).start()

    scope = jax.named_scope

    @pl.when(boss)
    def _():
        for number in (*range(2), 2 * kinds, 2 * kinds + 1, *range(2, 2 * kinds)):
            load(number).start()

    with scope("vectors"):
        for i, vector in enumerate((norm_gain, down_scale)):
            gains[i : i + 1, :] = vector[...].reshape(1, width)

        @pl.when(boss)
        def _():
            for i, (taps, scale, bias) in enumerate(
                ((value_taps, value_scale, value_bias), (gate_taps, gate_scale, gate_bias))
            ):
                along[3 * i : 3 * i + 3, :] = taps[...] * scale[...].reshape(1, units)
                along[6 + i : 7 + i, :] = bias[...].reshape(1, units)

    amounts = [many[k] + (1 if left_over[k] else 0) for k in range(kinds)]
    first = ("wide", 0) if many[0] else ("rest", 0)

    def others(body):
        if many[0] > 1:

            def one(q, carry):
                body("wide", q)
                return carry

            lax.fori_loop(1, many[0], one, 0)
        if left_over[0] and many[0]:
            body("rest", 0)

    def each(name, q, body):
        for r in range(CUT):
            body(piece(name, 0, q, r))

    with scope("cast_first"):

        @pl.when(boss)
        def _():
            loaded(kinds - 1)
            cast_up(kinds - 1, 0, amounts[-1])

    with scope("barrier"):
        sides = (here == 0).astype(jnp.int32) + (here == line - 1).astype(jnp.int32)
        pl.semaphore_wait(barrier, parts * peers - 1 + 2 - sides)
    with scope("send_first"):
        if lent:

            @pl.when(both(boss, end))
            def _():
                load(2 * kinds).wait()
                lend().start()

        pieces_up(kinds - 1, own_line)

        @pl.when(boss)
        def _():
            pl.when(inner if lent else boss)(lambda: load(2 * kinds).wait())
            swap(0).start()
            pl.when(jnp.logical_not(helper) if lent else boss)(lambda: swap(1).start())
            vectors().start()

        pieces_up(kinds - 1, own_across)
    with scope("cast_rest"):
        if lent:

            @pl.when(boss)
            def _():
                loaded(0)
                cast_up(0, 0, 1)

            each(*first, own_line)
        pl.when(boss)(lambda: load(2 * kinds + 1).wait())
        if lent:
            pl.when(boss)(lambda: cast_down(1))
            pieces_down(1, lambda which: own_line(which, True))
            pl.when(boss)(lambda: cast_up(0, 1, amounts[0]))
            others(lambda name, q: each(name, q, lambda which: own_line(which, True)))
            pieces_up(0, own_across)
        pl.when(boss)(lambda: cast_down(0))
        pieces_down(0, lambda which: own_line(which, True))
        for kind in reversed(range(kinds)):
            pieces_down(kind, own_across)

    with scope("normalize"):
        pl.when(boss)(lambda: normalize(token_load, normed))

    last = owner_at(line - 1)

    def nearer(name, q):
        with scope("a_near"):
            each(name, q, at_home)
            for i in reversed(range(1, line - 1)):
                each(name, q, lambda which: arrive(which, owner_at(i)))

    def farthest(name, q):
        with scope("a_far"):
            each(name, q, lambda which: arrive(which, last))

    if lent:
        with scope("relay"):
            pl.when(helper)(relay)

        def b_near(which):
            for i in range(1, line - 1):
                arrive(which, owner_at(i))

        with scope("b_near"):
            pieces_up(1, b_near)

    with scope("a_first"):
        each(*first, at_home)
        for i in reversed(range(1, line - 1)):
            each(*first, lambda which: arrive(which, owner_at(i)))
    if lent:
        others(lambda name, q: each(name, q, lambda which: own_line(which, False)))

    with scope("other_tokens"):

        @pl.when(other)
        def _():
            vectors().wait_recv()
            swap(0).wait_recv()
            swap(1).wait_recv()
            normalize(raw, normed)

    if lent:

        def b_own():
            groups(1, lambda name, q: up(1, name, q, normed, hidden[1]))

        with scope("b_far"):
            pieces_up(1, at_home)
            pieces_up(1, lambda which: arrive(which, last))
        with scope("b_own"):
            pl.when(both(boss, inner))(b_own)

        def c_early():
            with scope("c_early"):
                pieces_down(1, at_home)
                pieces_down(1, lambda which: arrive_here(which, owner_at(1)))

        pl.when(boss)(c_early)
        with scope("guest_wait"):
            pl.when(helper)(welcome)
        pl.when(boss)(lambda: farthest(*first))
        with scope("b_guest"):

            @pl.when(helper)
            def _():
                groups(1, lambda name, q: up(1, name, q, guest_normed, guest_hidden))

    def early_folds():
        def one(n, carry):
            guest_fold(slice_at(n))
            return carry

        with scope("early_folds"):
            lax.fori_loop(0, 2 * slices, one, 0)

    def guest_early():
        with scope("guest_early"):
            pieces_down(1, lambda which: pass_along(which, owner_at(1)))

            def early(j, carry):
                guest_project(slice_at(j))
                return carry

            lax.fori_loop(0, 2 * slices, early, 0)

    if lent:
        pl.when(other)(c_early)
        pl.when(other)(guest_early)
    others(nearer)
    if lent:
        pl.when(boss)(guest_early)
        pl.when(other)(lambda: farthest(*first))
    else:
        farthest(*first)
    if lent:
        with scope("b_own"):
            pl.when(both(other, inner))(b_own)
        pl.when(other)(early_folds)


    def own_down(begin, stop):
        for r in range(begin, stop):
            for kind in reversed(range(kinds)):
                own_line(piece("down", kind, 0, r), False)

    def own_up(name, q):
        if not lent:
            final = q == many[0] - 1 if not left_over[0] else here < (line if name == "rest" else 0)
            pl.when(final)(lambda: own_down(0, slices))
        if name == "wide" or many[0]:
            pl.when(jnp.logical_or(name == "rest", q > 0))(lambda: farthest(name, q))
        with scope("a_own"):
            up(0, name, q, normed, hidden[0])

    groups(0, own_up)
    with scope("c_near"):
        pieces_down(0, lambda which: arrive(which, owner_at(1)))
    if lent:
        own_down(0, slices)
        pl.when(boss)(early_folds)

    def collect(at, slots):
        columns = pl.ds(pl.multiple_of(at * thin, thin), thin)
        total = gathered(landed, at, slots, sum_recv)

        def keep(amount):
            out[:, columns] = (amount * gains[1:2, columns]).astype(jnp.bfloat16)

        if lent:

            @pl.when(end)
            def _():
                back(at).wait_recv()
                keep(total + returned[at].astype(jnp.float32))

            pl.when(inner)(lambda: keep(total))
        else:
            keep(total)

    total_slices = line * slices
    near = 2 * slices

    clip = lambda value, most: lax.clamp(0, value, most)

    def own_folds(j):
        return lax.min(
            clip(2 * (j - near + 1), near) + clip(j - near - slices + 1, total_slices), folded
        )

    def collects(j):
        return jnp.where(j < near + 2, 0, own_folds(j - 2))

    def guest_folds(j):
        late = jnp.where(j < near + slices, 1, 0)
        return near + clip(j - near - late, folded - near)

    def give_backs(j):
        two_steps = lax.min(2 * (j - near + 1), guest_folds(j - 1))
        return jnp.where(j < near, 0, two_steps + clip(j - folded, slices))

    def advance(done, j, body, base=0):
        def one(n, carry):
            body(n)
            return carry

        lax.fori_loop(jnp.where(j > 0, done(j - 1), base), done(j), one, 0)

    def complete(done, everything, body):
        def one(n, carry):
            body(n)
            return carry

        lax.fori_loop(done(jnp.int32(total_slices - 1)), everything, one, 0)

    one_fold = lambda n: fold(slice_at(n))
    one_collect = lambda n: collect(slice_at(n), pairs)
    one_guest_fold = lambda n: guest_fold(slice_at(n))

    def one_give_back(n):
        pl.when(n < folded)(lambda: give_back(slice_at(n), parts))
        pl.when(n >= folded)(lambda: give_back(slice_at(n), peers))


    def finish_line(j, carry):
        p, r = j // slices, j % slices
        owner = turn(p)
        for kind in reversed(range(kinds)):
            which = piece("down", kind, 0, r)
            with scope(f"c_arrive#k={kind}"):
                if not kind:
                    pl.when(p == 0)(lambda: at_home(which))
                pl.when(p > 1)(lambda: arrive(which, owner))
            if kind:
                with scope("c_guest"):
                    pl.when(p > 1)(lambda: guest_project(owner * slices + r, p == line - 1))
        with scope("c_own"):
            project(owner * slices + r, p == line - 1)
        if lent:
            with scope("guest_fold"):
                advance(guest_folds, j, one_guest_fold, near)
        with scope("fold"):
            advance(own_folds, j, one_fold)
        if lent:
            with scope("give_back"):
                advance(give_backs, j, one_give_back)
        with scope("collect"):
            advance(collects, j, one_collect)
        return carry

    lax.fori_loop(0, total_slices, finish_line, 0)
    if lent:
        with scope("guest_fold_rest"):
            complete(guest_folds, folded, one_guest_fold)
        with scope("give_rest"):
            complete(give_backs, total_slices, one_give_back)
    with scope("fold_rest"):
        complete(own_folds, folded, one_fold)
    with scope("collect_rest"):
        complete(collects, folded, one_collect)

    def collect_last(n, carry):
        with scope("collect_last"):
            collect(slice_at(n), peers)
        return carry

    lax.fori_loop(folded, total_slices, collect_last, 0)

    def departed(name, kind, amount, lane):
        part = store_rows(name, kind, pl.ds(0, amount * held))
        pltpu.make_async_copy(part, part, send_sem.at[stores[name, kind], lane]).wait()

    with scope("left"):
        pl.when(boss)(lambda: handed(landed.at[:, pl.ds(0, peers - 1)], sum_send))

        @pl.when(other)
        def _():
            handed(landed.at[pl.ds(0, slices)], sum_send)
            if folded:
                handed(x_stage.at[pl.ds(0, folded)], x_send)


        @pl.when(boss)
        def _():
            swap(0).wait_send()
            swap(1).wait_send()
            vectors().wait_send()
            for kind in range(kinds):
                for name, there in (("wide", many[kind]), ("rest", left_over[kind]), ("down", 1)):
                    if there:
                        for lane, direction in ((0, 1), (1, -1)):
                            amount = here + 1 if direction > 0 else line - here
                            for some in range(1, line):
                                pl.when(both(amount == some, further(kind, direction)))(
                                    lambda: departed(name, kind, some, lane)
                                )
                        pl.when(used(kind))(lambda: departed(name, kind, line, 2))

        if lent:
            pl.when(both(boss, end))(lambda: lend().wait_send())

            @pl.when(helper)
            def _():
                pl.when(boss)(lambda: pass_across().wait_send())
                for k in range(1, pairs):
                    pass_on(k).wait_send()
                if pairs > 1:
                    handed(y_stage.at[pl.ds(0, folded), pl.ds(0, pairs - 1)], y_send)

                def guests_left(in_two, at_once):
                    handed(guest_landed.at[pl.ds(0, folded), pl.ds(0, in_two)], guest_sum_send)
                    handed(guest_landed.at[pl.ds(0, slices), pl.ds(0, at_once)], guest_direct)

                pl.when(boss)(lambda: guests_left(parts - 1, peers - 1))
                pl.when(other)(lambda: guests_left(parts, peers))
                pltpu.make_async_copy(summed, summed, back_send).wait()


def solution(mesh):
    parts, line, peers = mesh.shape["grp"], mesh.shape["fs"], mesh.shape["tp"]

    def local(*arrays):
        rows, width = arrays[0].shape
        held, units = arrays[2].shape
        kept = rows // peers
        pairs = peers // parts
        lent = units * 6 // 11 // 128 * 128 if line >= 4 and peers > 1 else 0
        slices = 4 if held % 512 == 0 else 1
        thin = held // slices
        half, full = jnp.bfloat16, jnp.float32
        spans = (units - lent, lent) if lent else (units,)
        dma = pltpu.SemaphoreType.DMA
        scratch = [
            pltpu.VMEM((span // WIDE, 2, width, WIDE), half) for span in spans if span // WIDE
        ]
        scratch += [pltpu.VMEM((2, width, span % WIDE), half) for span in spans if span % WIDE]
        scratch += [pltpu.VMEM((width, span), half) for span in spans]
        scratch += [pltpu.VMEM((rows, span), half) for span in spans]
        pieces = sum(pl.cdiv(span, WIDE) * CUT + slices for span in spans)
        scratch += [
            pltpu.VMEM((held, units), full),
            pltpu.VMEM((held, units), full),
            pltpu.VMEM((held, units), full),
            pltpu.VMEM((rows, width), half),
            pltpu.VMEM((rows, width), half),
            pltpu.VMEM((rows, width), half),
            pltpu.VMEM((8, units), full),
            pltpu.VMEM((2, width), full),
            pltpu.VMEM((line * slices, rows, thin), half),
            pltpu.VMEM((line * slices, peers, kept, thin), half),
            pltpu.VMEM((line * slices, rows, thin), half),
            dma((3 * len(spans), 3)),
            dma((pieces, line)),
            dma((2 * len(spans) + 2,)),
            dma((4,)),
            dma((2,)),
            dma,
            dma((line * slices,)),
            dma,
            dma((line * slices,)),
        ]
        if lent:
            scratch += [
                pltpu.VMEM((rows, width), half),
                pltpu.VMEM((rows, width), half),
                pltpu.VMEM((rows, lent), half),
                pltpu.VMEM((line * slices, rows, thin), half),
                pltpu.VMEM((line * slices, peers, kept, thin), half),
                pltpu.VMEM((line * slices, pairs, parts * kept, thin), half),
                pltpu.VMEM((line * slices, kept, thin), half),
                pltpu.VMEM((line * slices, kept, thin), half),
                dma((pairs + 1,)),
                dma((pairs,)),
                dma,
                dma((line * slices,)),
                dma,
                dma,
                dma((line * slices,)),
                dma,
                dma((line * slices,)),
            ]
        return pl.pallas_call(
            functools.partial(kernel, parts, line, peers, lent, slices),
            out_shape=pltpu.VMEM((kept, width), half),
            in_specs=[
                pl.BlockSpec(memory_space=pl.ANY if i in (0, 2, 3, 4) else pltpu.VMEM)
                for i in range(12)
            ],
            out_specs=pl.BlockSpec(memory_space=pltpu.VMEM),
            scratch_shapes=scratch,
            compiler_params=pltpu.CompilerParams(
                collective_id=0, has_side_effects=True, vmem_limit_bytes=62 * 1024 * 1024
            ),
        )(*arrays)

    return jax.shard_map(
        local,
        mesh=mesh,
        in_specs=(
            P(("grp", "fs"), None),
            P(),
            P("fs", "tp"),
            P("fs", "tp"),
            P("fs", "tp"),
            P("tp"),
            P("tp"),
            P(),
            P(None, "tp"),
            P(None, "tp"),
            P("tp"),
            P("tp"),
        ),
        out_specs=P(("grp", "fs", "tp"), None),
        check_vma=False,
    )
```

```python
import functools

import jax
import jax.numpy as jnp
from jax import lax
from jax.experimental import pallas as pl
from jax.experimental.pallas import tpu as pltpu
from jax.sharding import PartitionSpec as P

MESH = pl.DeviceIdType.MESH
WIDE = 256
CUT = 2


def kernel(
    parts,
    line,
    peers,
    lent,
    slices,
    tokens,
    norm_gain,
    value_weight,
    gate_weight,
    down_weight,
    value_scale,
    gate_scale,
    down_scale,
    value_taps,
    gate_taps,
    value_bias,
    gate_bias,
    out,
    *scratch,
):
    group, here, me = lax.axis_index("grp"), lax.axis_index("fs"), lax.axis_index("tp")
    scratch = list(scratch)
    take = lambda count: [scratch.pop(0) for _ in range(count)]
    kinds = 2 if lent else 1
    rows, width = tokens.shape
    held, units = value_weight.shape
    thin = held // slices
    kept = rows // peers
    pairs = peers // parts
    base = (0, units - lent)
    span = (units - lent, lent)
    many = [span[k] // WIDE for k in range(kinds)]
    left_over = [span[k] % WIDE for k in range(kinds)]
    wide = [take(1)[0] if many[k] else None for k in range(kinds)]
    rest = [take(1)[0] if left_over[k] else None for k in range(kinds)]
    down = take(kinds)
    hidden = take(kinds)
    value_load, gate_load, down_load, token_load = take(4)
    raw, normed, along, gains, partial, landed, x_stage = take(7)
    send_sem, recv_sem, load_sem, token_sem, along_sem = take(5)
    sum_send, sum_recv, x_send, x_recv = take(4)
    if lent:
        guest, guest_normed, guest_hidden, guest_partial, guest_landed, y_stage = take(6)
        summed, returned, guest_send, guest_recv, back_send, back_recv = take(6)
        guest_sum_send, guest_direct, guest_sum_recv, y_send, y_recv = take(5)

    pair = lax.div(me, parts)
    core = lax.rem(me, parts)
    boss = core == group
    other = jnp.logical_not(boss)
    block = pair * parts + group
    sibling = pair * parts + lax.rem(core + 1, parts)
    end = jnp.logical_or(here == 0, here == line - 1)
    inner = jnp.logical_not(end)
    helper = jnp.logical_and(inner, jnp.logical_or(here == 1, here == line - 2))
    mate = jnp.where(end, jnp.where(here == 0, 1, line - 2), jnp.where(here == 1, 0, line - 1))
    both = jnp.logical_and

    barrier = pltpu.get_barrier_semaphore()

    def greet(target):
        pl.semaphore_signal(barrier, inc=1, device_id=target, device_id_type=MESH)

    pl.when(here > 0)(lambda: greet({"fs": here - 1}))
    pl.when(here < line - 1)(lambda: greet({"fs": here + 1}))
    for j in range(parts):
        for k in range(peers):
            if j or k:
                greet({"grp": lax.rem(group + j, parts), "tp": lax.rem(me + k, peers)})

    def owner_at(i):
        near = jnp.where(here < line // 2, here, line - 1 - here)
        turned = jnp.where(i % 2 == 1, near - (i + 1) // 2, near + i // 2)
        first = jnp.where(i > 2 * near, i, turned)
        return jnp.where(here < line // 2, first, line - 1 - first)

    def turn(p):
        if line != 4:
            return owner_at(p)
        return owner_at(jnp.where(p < 2, p, 5 - p))

    def slice_at(j):
        return turn(j // slices) * slices + j % slices

    numbers, stores = {}, {}
    count = 0
    for k in range(kinds):
        for name, amount in (("wide", many[k] * CUT), ("rest", CUT), ("down", slices)):
            stores[name, k] = len(stores)
            numbers[name, k] = count
            count += amount if name != "rest" or left_over[k] else 0

    def store_rows(name, kind, taken):
        if name == "wide":
            return wide[kind].at[:, :, taken, :]
        if name == "rest":
            return rest[kind].at[:, taken, :]
        return down[kind].at[taken, :]

    def piece(name, kind, q, r):
        cut = slices if name == "down" else CUT

        def ref(owner):
            part = held // cut
            taken = pl.ds(pl.multiple_of(owner * held + r * part, part), part)
            return wide[kind].at[q, :, taken, :] if name == "wide" else store_rows(name, kind, taken)

        return numbers[name, kind] + q * CUT + r, kind, ref, stores[name, kind]

    def groups(kind, body):
        if many[kind]:

            def one(q, carry):
                body("wide", q)
                return carry

            lax.fori_loop(0, many[kind], one, 0)
        if left_over[kind]:
            body("rest", 0)

    def copy(which, owner, direction):
        number, kind, ref, store = which
        if direction is None:
            target, lane = {"tp": sibling}, 2
        else:
            target = {"fs": lax.clamp(0, here + direction, line - 1)}
            lane = jnp.where(direction > 0, 0, 1)
        return pltpu.make_async_remote_copy(
            src_ref=ref(owner),
            dst_ref=ref(owner),
            send_sem=send_sem.at[store, lane],
            recv_sem=recv_sem.at[number, owner],
            device_id=target,
            device_id_type=MESH,
        )

    def used(kind):
        return inner if kind else here >= 0

    def further(kind, direction):
        there = here + direction
        return both(there >= kind, there <= line - 1 - kind)

    def toward_end(direction):
        there = here + direction
        return jnp.logical_or(end, jnp.logical_or(there == 0, there == line - 1))

    def own_line(which, early=None):
        for direction in (1, -1):
            go = both(boss, further(which[1], direction))
            if early is True:
                go = both(go, toward_end(direction))
            elif early is False:
                go = both(go, jnp.logical_not(toward_end(direction)))
            pl.when(go)(lambda: copy(which, here, direction).start())

    def own_across(which):
        pl.when(both(boss, used(which[1])))(lambda: copy(which, here, None).start())

    def arrive_here(which, owner):
        @pl.when(used(which[1]))
        def _():
            copy(which, owner, None).wait_recv()
            pl.when(boss)(lambda: copy(which, owner, None).start())

    def pass_along(which, owner):
        direction = jnp.where(owner < here, 1, -1)
        go = both(both(boss, used(which[1])), further(which[1], direction))
        pl.when(go)(lambda: copy(which, owner, direction).start())

    def arrive(which, owner):
        direction = jnp.where(owner < here, 1, -1)

        @pl.when(used(which[1]))
        def _():
            copy(which, owner, None).wait_recv()

            @pl.when(boss)
            def _():
                pl.when(further(which[1], direction))(lambda: copy(which, owner, direction).start())
                copy(which, owner, None).start()

    def at_home(which):
        pl.when(both(other, used(which[1])))(lambda: copy(which, here, None).wait_recv())

    def pieces_up(kind, body):
        def group_body(name, q):
            for r in range(CUT):
                body(piece(name, kind, q, r))

        groups(kind, group_body)

    def pieces_down(kind, body):
        for r in range(slices):
            body(piece("down", kind, 0, r))

    def cast_rows(source, columns, store):
        step = min(held, 64)

        def body(i, carry):
            taken = pl.ds(pl.multiple_of(i * step, step), step)
            target = pl.ds(pl.multiple_of(here * held + i * step, step), step)
            store(target, source[taken, columns].astype(jnp.bfloat16))
            return carry

        lax.fori_loop(0, held // step, body, 0)

    def load(number):
        if number < 2 * kinds:
            kind = kinds - 1 - number // 2
            columns = pl.ds(base[kind], span[kind])
            source, target = ((value_weight, value_load), (gate_weight, gate_load))[number % 2]
            source, target = source.at[:, columns], target.at[:, columns]
        elif number == 2 * kinds:
            source, target = tokens, token_load
        else:
            source, target = down_weight, down_load
        return pltpu.make_async_copy(source, target, load_sem.at[number])

    def loaded(kind):
        for m in range(2):
            load(2 * (kinds - 1 - kind) + m).wait()

    def cast_up(kind, begin, stop):
        for m, source in enumerate((value_load, gate_load)):
            for q in range(begin, stop):
                first = base[kind] + q * WIDE

                def store(target, values):
                    if q < many[kind]:
                        wide[kind][q, m, target, :] = values
                    else:
                        rest[kind][m, target, :] = values

                cast_rows(source, slice(first, min(first + WIDE, base[kind] + span[kind])), store)

    def cast_down(kind):
        def store(target, values):
            down[kind][target, :] = values

        cast_rows(down_load, slice(base[kind], base[kind] + span[kind]), store)

    def normalize(source, target):
        step = min(rows, 64)

        def body(i, carry):
            taken = pl.ds(pl.multiple_of(i * step, step), step)
            floated = source[taken, :].astype(jnp.float32)
            mean = jnp.mean(floated * floated, axis=-1, keepdims=True)
            target[taken, :] = (floated * lax.rsqrt(mean + 1e-06) * gains[0:1, :]).astype(
                jnp.bfloat16
            )
            return carry

        lax.fori_loop(0, rows // step, body, 0)

    def swap(part):
        taken = pl.ds(part * (rows // 2), rows // 2)
        return pltpu.make_async_remote_copy(
            src_ref=token_load.at[taken, :],
            dst_ref=raw.at[taken, :],
            send_sem=token_sem.at[part],
            recv_sem=token_sem.at[2 + part],
            device_id={"grp": lax.rem(group + 1, parts)},
            device_id_type=MESH,
        )

    def vectors():
        return pltpu.make_async_remote_copy(
            src_ref=along,
            dst_ref=along,
            send_sem=along_sem.at[0],
            recv_sem=along_sem.at[1],
            device_id={"tp": sibling},
            device_id_type=MESH,
        )

    share = rows // pairs

    def portion(ref):
        return ref.at[pl.ds(pl.multiple_of(pair * share, share), share), :]

    def guest_copy(source, slot, target):
        return pltpu.make_async_remote_copy(
            src_ref=portion(source),
            dst_ref=portion(guest),
            send_sem=guest_send.at[slot],
            recv_sem=guest_recv.at[pair],
            device_id=target,
            device_id_type=MESH,
        )

    def lend():
        return guest_copy(token_load, pairs, {"fs": mate})

    def pass_on(k):
        return guest_copy(guest, k, {"tp": lax.rem(me + k * parts, peers)})

    def pass_across():
        return guest_copy(guest, 0, {"grp": lax.rem(group + 1, parts)})

    def relay():
        lend().wait_recv()
        pl.when(boss)(lambda: pass_across().start())
        pl.when(boss)(lambda: swap(1).start())
        for k in range(1, pairs):
            pass_on(k).start()

    def welcome():
        for k in range(1, pairs):
            from_pair = lax.rem(pair + k, pairs)
            landed_share = guest.at[pl.ds(pl.multiple_of(from_pair * share, share), share), :]
            pltpu.make_async_copy(landed_share, landed_share, guest_recv.at[from_pair]).wait()
        normalize(guest, guest_normed)

    def causal(weight, tap, bias, source, outer):
        up = jnp.dot(source[...], weight[...], preferred_element_type=jnp.float32)
        position = lax.broadcasted_iota(jnp.int32, up.shape, 0)
        one = jnp.where(position >= 1, pltpu.roll(up, 1, axis=0), 0.0)
        two = jnp.where(position >= 2, pltpu.roll(up, 2, axis=0), 0.0)
        return (
            along[tap : tap + 1, outer] * two
            + along[tap + 1 : tap + 2, outer] * one
            + along[tap + 2 : tap + 3, outer] * up
            + along[bias : bias + 1, outer]
        )

    def up(kind, name, q, source, keep):
        weights = wide[kind].at[q] if name == "wide" else rest[kind]
        extent = WIDE if name == "wide" else left_over[kind]
        first = q * WIDE if name == "wide" else many[kind] * WIDE
        if name == "wide":
            first = pl.multiple_of(first, WIDE)
            outer = pl.ds(pl.multiple_of(base[kind] + first, 128), extent)
        else:
            outer = pl.ds(base[kind] + first, extent)
        value = causal(weights.at[0], 0, 6, source, outer)
        gate = causal(weights.at[1], 3, 7, source, outer)
        keep[:, pl.ds(first, extent)] = (gate / (1.0 + jnp.exp(-gate)) * value).astype(jnp.bfloat16)

    def through(kind, activations, owner):
        shard = down[kind][pl.ds(pl.multiple_of(owner * thin, thin), thin), :]
        return lax.dot_general(
            activations[...], shard, (((1,), (1,)), ((), ())), preferred_element_type=jnp.float32
        )

    def hand(source, target, at, slot, to_group, peer, sent, received):
        return pltpu.make_async_remote_copy(
            src_ref=source.at[at, pl.ds(pl.multiple_of(peer * kept, kept), kept), :],
            dst_ref=target.at[at, slot],
            send_sem=sent,
            recv_sem=received.at[at],
            device_id={"grp": to_group, "tp": peer},
            device_id_type=MESH,
        )

    mine = pl.ds(pl.multiple_of(me * kept, kept), kept)
    folded = (line - 1) * slices

    def direct(source, target, at, sent, received):
        for k in range(peers):
            peer = lax.rem(me + k, peers)
            copy_out = hand(source, target, at, block, core, peer, sent, received)
            pl.when(other if k == 0 else here >= 0)(lambda: copy_out.start())

        @pl.when(boss)
        def _():
            target[at, block] = source[at, mine, :]

    def across(at):
        return pltpu.make_async_remote_copy(
            src_ref=partial.at[at],
            dst_ref=x_stage.at[at],
            send_sem=x_send,
            recv_sem=x_recv.at[at],
            device_id={"grp": lax.rem(group + 1, parts)},
            device_id_type=MESH,
        )

    def fold(at):
        @pl.when(boss)
        def _():
            across(at).wait_recv()
            total = partial[at].astype(jnp.float32) + x_stage[at].astype(jnp.float32)
            partial[at] = total.astype(jnp.bfloat16)
            for k in range(1, peers):
                peer = lax.rem(me + k, peers)
                hand(partial, landed, at, pair, group, peer, sum_send, sum_recv).start()
            landed[at, pair] = partial[at, mine, :]

    pair_rows = parts * kept

    def beside(at, k):
        there = pl.multiple_of(lax.rem(pair + k, pairs) * pair_rows, pair_rows)
        return pltpu.make_async_remote_copy(
            src_ref=guest_partial.at[at, pl.ds(there, pair_rows), :],
            dst_ref=y_stage.at[at, k - 1],
            send_sem=y_send,
            recv_sem=y_recv.at[at],
            device_id={"tp": lax.rem(me + k * parts, peers)},
            device_id_type=MESH,
        )

    def guest_fold(at):
        ours = pl.ds(pl.multiple_of(pair * pair_rows, pair_rows), pair_rows)

        @pl.when(helper)
        def _():
            if pairs > 1:
                staged = y_stage.at[at, pl.ds(0, pairs - 1)]
                pltpu.make_async_copy(staged, staged, y_recv.at[at]).wait()
                total = guest_partial[at, ours, :].astype(jnp.float32)
                for k in range(1, pairs):
                    total = total + y_stage[at, k - 1].astype(jnp.float32)
                guest_partial[at, ours, :] = total.astype(jnp.bfloat16)
            for k in range(parts):
                peer = pair * parts + lax.rem(core + k, parts)
                copy_out = hand(
                    guest_partial, guest_landed, at, group, core, peer, guest_sum_send, guest_sum_recv
                )
                pl.when(other if k == 0 else here >= 0)(lambda: copy_out.start())

            @pl.when(boss)
            def _():
                guest_landed[at, group] = guest_partial[at, mine, :]

    def gathered(target, at, slots, received):
        def some(amount):
            if amount:
                part = target.at[at, pl.ds(0, amount)]
                pltpu.make_async_copy(part, part, received.at[at]).wait()

        pl.when(boss)(lambda: some(slots - 1))
        pl.when(other)(lambda: some(slots))
        total = target[at, 0].astype(jnp.float32)
        for k in range(1, slots):
            total = total + target[at, k].astype(jnp.float32)
        return total

    def handed(part, sent):
        pltpu.make_async_copy(part, part, sent).wait()

    def project(owner, is_last):
        if lent:

            @pl.when(inner)
            def _():
                partial[owner] = (through(0, hidden[0], owner) + through(1, hidden[1], owner)).astype(
                    jnp.bfloat16
                )

            @pl.when(end)
            def _():
                partial[owner] = through(0, hidden[0], owner).astype(jnp.bfloat16)

        else:
            partial[owner] = through(0, hidden[0], owner).astype(jnp.bfloat16)
        pl.when(is_last)(lambda: direct(partial, landed, owner, sum_send, sum_recv))
        pl.when(both(other, jnp.logical_not(is_last)))(lambda: across(owner).start())

    def guest_project(owner, is_last=None):
        @pl.when(helper)
        def _():
            guest_partial[owner] = through(1, guest_hidden, owner).astype(jnp.bfloat16)
            def besides():
                for k in range(1, pairs):
                    beside(owner, k).start()

            if is_last is None:
                besides()
            else:
                pl.when(jnp.logical_not(is_last))(besides)
                pl.when(is_last)(
                    lambda: direct(guest_partial, guest_landed, owner, guest_direct, guest_sum_recv)
                )

    def back(owner):
        return pltpu.make_async_remote_copy(
            src_ref=summed.at[owner],
            dst_ref=returned.at[owner],
            send_sem=back_send,
            recv_sem=back_recv.at[owner],
            device_id={"fs": mate},
            device_id_type=MESH,
        )

    def give_back(owner, slots):
        @pl.when(helper)
        def _():
            summed[owner] = gathered(guest_landed, owner, slots, guest_sum_recv).astype(jnp.bfloat16)
            back(owner).start()

    scope = jax.named_scope

    @pl.when(boss)
    def _():
        for number in (*range(2), 2 * kinds, 2 * kinds + 1, *range(2, 2 * kinds)):
            load(number).start()

    with scope("vectors"):
        for i, vector in enumerate((norm_gain, down_scale)):
            gains[i : i + 1, :] = vector[...].reshape(1, width)

        @pl.when(boss)
        def _():
            for i, (taps, scale, bias) in enumerate(
                ((value_taps, value_scale, value_bias), (gate_taps, gate_scale, gate_bias))
            ):
                along[3 * i : 3 * i + 3, :] = taps[...] * scale[...].reshape(1, units)
                along[6 + i : 7 + i, :] = bias[...].reshape(1, units)

    amounts = [many[k] + (1 if left_over[k] else 0) for k in range(kinds)]
    first = ("wide", 0) if many[0] else ("rest", 0)

    def others(body):
        if many[0] > 1:

            def one(q, carry):
                body("wide", q)
                return carry

            lax.fori_loop(1, many[0], one, 0)
        if left_over[0] and many[0]:
            body("rest", 0)

    def each(name, q, body):
        for r in range(CUT):
            body(piece(name, 0, q, r))

    with scope("cast_first"):

        @pl.when(boss)
        def _():
            loaded(kinds - 1)
            cast_up(kinds - 1, 0, amounts[-1])

    with scope("barrier"):
        sides = (here == 0).astype(jnp.int32) + (here == line - 1).astype(jnp.int32)
        pl.semaphore_wait(barrier, parts * peers - 1 + 2 - sides)
    with scope("send_first"):
        if lent:

            @pl.when(both(boss, end))
            def _():
                load(2 * kinds).wait()
                lend().start()

        pieces_up(kinds - 1, own_line)

        @pl.when(boss)
        def _():
            pl.when(inner if lent else boss)(lambda: load(2 * kinds).wait())
            swap(0).start()
            pl.when(jnp.logical_not(helper) if lent else boss)(lambda: swap(1).start())
            vectors().start()

        pieces_up(kinds - 1, own_across)
    with scope("cast_rest"):
        if lent:

            @pl.when(boss)
            def _():
                loaded(0)
                cast_up(0, 0, 1)

            each(*first, own_line)
        pl.when(boss)(lambda: load(2 * kinds + 1).wait())
        if lent:
            pl.when(boss)(lambda: cast_down(1))
            pieces_down(1, lambda which: own_line(which, True))
            pl.when(boss)(lambda: cast_up(0, 1, amounts[0]))
            others(lambda name, q: each(name, q, lambda which: own_line(which, True)))
            pieces_up(0, own_across)
        pl.when(boss)(lambda: cast_down(0))
        pieces_down(0, lambda which: own_line(which, True))
        for kind in reversed(range(kinds)):
            pieces_down(kind, own_across)

    with scope("normalize"):
        pl.when(boss)(lambda: normalize(token_load, normed))

    last = owner_at(line - 1)

    def nearer(name, q):
        with scope("a_near"):
            each(name, q, at_home)
            for i in reversed(range(1, line - 1)):
                each(name, q, lambda which: arrive(which, owner_at(i)))

    def farthest(name, q):
        with scope("a_far"):
            each(name, q, lambda which: arrive(which, last))

    if lent:
        with scope("relay"):
            pl.when(helper)(relay)

        def b_near(which):
            for i in range(1, line - 1):
                arrive(which, owner_at(i))

        with scope("b_near"):
            pieces_up(1, b_near)

    with scope("a_first"):
        each(*first, at_home)
        for i in reversed(range(1, line - 1)):
            each(*first, lambda which: arrive(which, owner_at(i)))
    if lent:
        others(lambda name, q: each(name, q, lambda which: own_line(which, False)))

    with scope("other_tokens"):

        @pl.when(other)
        def _():
            vectors().wait_recv()
            swap(0).wait_recv()
            swap(1).wait_recv()
            normalize(raw, normed)

    if lent:

        def b_own():
            groups(1, lambda name, q: up(1, name, q, normed, hidden[1]))

        with scope("b_far"):
            pieces_up(1, at_home)
            pieces_up(1, lambda which: arrive(which, last))
        with scope("b_own"):
            pl.when(both(boss, inner))(b_own)

        def c_early():
            with scope("c_early"):
                pieces_down(1, at_home)
                pieces_down(1, lambda which: arrive_here(which, owner_at(1)))

        pl.when(boss)(c_early)
        with scope("guest_wait"):
            pl.when(helper)(welcome)
        pl.when(boss)(lambda: farthest(*first))
        with scope("b_guest"):

            @pl.when(helper)
            def _():
                groups(1, lambda name, q: up(1, name, q, guest_normed, guest_hidden))

    def early_folds():
        def one(n, carry):
            guest_fold(slice_at(n))
            return carry

        with scope("early_folds"):
            lax.fori_loop(0, 2 * slices, one, 0)

    def guest_early():
        with scope("guest_early"):
            pieces_down(1, lambda which: pass_along(which, owner_at(1)))

            def early(j, carry):
                guest_project(slice_at(j))
                return carry

            lax.fori_loop(0, 2 * slices, early, 0)

    if lent:
        pl.when(other)(c_early)
        pl.when(other)(guest_early)
    others(nearer)
    if lent:
        pl.when(boss)(guest_early)
        pl.when(other)(lambda: farthest(*first))
    else:
        farthest(*first)
    if lent:
        with scope("b_own"):
            pl.when(both(other, inner))(b_own)
        pl.when(other)(early_folds)


    def own_down(begin, stop):
        for r in range(begin, stop):
            for kind in reversed(range(kinds)):
                own_line(piece("down", kind, 0, r), False)

    def own_up(name, q):
        if not lent:
            final = q == many[0] - 1 if not left_over[0] else here < (line if name == "rest" else 0)
            pl.when(final)(lambda: own_down(0, slices))
        if name == "wide" or many[0]:
            pl.when(jnp.logical_or(name == "rest", q > 0))(lambda: farthest(name, q))
        with scope("a_own"):
            up(0, name, q, normed, hidden[0])

    groups(0, own_up)
    with scope("c_near"):
        pieces_down(0, lambda which: arrive(which, owner_at(1)))
    if lent:
        own_down(0, slices)
        pl.when(boss)(early_folds)

    def collect(at, slots):
        columns = pl.ds(pl.multiple_of(at * thin, thin), thin)
        total = gathered(landed, at, slots, sum_recv)

        def keep(amount):
            out[:, columns] = (amount * gains[1:2, columns]).astype(jnp.bfloat16)

        if lent:

            @pl.when(end)
            def _():
                back(at).wait_recv()
                keep(total + returned[at].astype(jnp.float32))

            pl.when(inner)(lambda: keep(total))
        else:
            keep(total)

    total_slices = line * slices
    near = 2 * slices

    clip = lambda value, most: lax.clamp(0, value, most)

    def own_folds(j):
        early = clip(2 * (j - near + 1), near)
        later = clip(2 * (j - near - slices + 1), total_slices)
        return lax.min(lax.min(early + later, folded), lax.max(j, 0))

    def collects(j):
        return jnp.where(j < near + 2, 0, own_folds(j - 2))

    def guest_folds(j):
        return near + clip(j - near - 1, folded - near)

    def give_backs(j):
        return jnp.where(j < near, 0, lax.min(2 * (j - near + 1), guest_folds(j - 2)))

    def advance(done, j, body, base=0):
        def one(n, carry):
            body(n)
            return carry

        lax.fori_loop(jnp.where(j > 0, done(j - 1), base), done(j), one, 0)

    def complete(done, everything, body):
        def one(n, carry):
            body(n)
            return carry

        lax.fori_loop(done(jnp.int32(total_slices - 1)), everything, one, 0)

    one_fold = lambda n: fold(slice_at(n))
    one_collect = lambda n: collect(slice_at(n), pairs)
    one_guest_fold = lambda n: guest_fold(slice_at(n))

    def one_give_back(n):
        pl.when(n < folded)(lambda: give_back(slice_at(n), parts))
        pl.when(n >= folded)(lambda: give_back(slice_at(n), peers))


    def finish_line(j, carry):
        p, r = j // slices, j % slices
        owner = turn(p)
        for kind in reversed(range(kinds)):
            which = piece("down", kind, 0, r)
            with scope(f"c_arrive#k={kind}"):
                if not kind:
                    pl.when(p == 0)(lambda: at_home(which))
                pl.when(p > 1)(lambda: arrive(which, owner))
            if kind:
                with scope("c_guest"):
                    pl.when(p > 1)(lambda: guest_project(owner * slices + r, p == line - 1))
        with scope("c_own"):
            project(owner * slices + r, p == line - 1)
        if lent:
            with scope("guest_fold"):
                advance(guest_folds, j, one_guest_fold, near)
        with scope("fold"):
            advance(own_folds, j, one_fold)
        if lent:
            with scope("give_back"):
                advance(give_backs, j, one_give_back)
        with scope("collect"):
            advance(collects, j, one_collect)
        return carry

    lax.fori_loop(0, total_slices, finish_line, 0)
    if lent:
        with scope("guest_fold_rest"):
            complete(guest_folds, folded, one_guest_fold)
        with scope("give_rest"):
            complete(give_backs, total_slices, one_give_back)
    with scope("fold_rest"):
        complete(own_folds, folded, one_fold)
    with scope("collect_rest"):
        complete(collects, folded, one_collect)

    def collect_last(n, carry):
        with scope("collect_last"):
            collect(slice_at(n), peers)
        return carry

    lax.fori_loop(folded, total_slices, collect_last, 0)

    def departed(name, kind, amount, lane):
        part = store_rows(name, kind, pl.ds(0, amount * held))
        pltpu.make_async_copy(part, part, send_sem.at[stores[name, kind], lane]).wait()

    with scope("left"):
        pl.when(boss)(lambda: handed(landed.at[:, pl.ds(0, peers - 1)], sum_send))

        @pl.when(other)
        def _():
            handed(landed.at[pl.ds(0, slices)], sum_send)
            if folded:
                handed(x_stage.at[pl.ds(0, folded)], x_send)


        @pl.when(boss)
        def _():
            swap(0).wait_send()
            swap(1).wait_send()
            vectors().wait_send()
            for kind in range(kinds):
                for name, there in (("wide", many[kind]), ("rest", left_over[kind]), ("down", 1)):
                    if there:
                        for lane, direction in ((0, 1), (1, -1)):
                            amount = here + 1 if direction > 0 else line - here
                            for some in range(1, line):
                                pl.when(both(amount == some, further(kind, direction)))(
                                    lambda: departed(name, kind, some, lane)
                                )
                        pl.when(used(kind))(lambda: departed(name, kind, line, 2))

        if lent:
            pl.when(both(boss, end))(lambda: lend().wait_send())

            @pl.when(helper)
            def _():
                pl.when(boss)(lambda: pass_across().wait_send())
                for k in range(1, pairs):
                    pass_on(k).wait_send()
                if pairs > 1:
                    handed(y_stage.at[pl.ds(0, folded), pl.ds(0, pairs - 1)], y_send)

                def guests_left(in_two, at_once):
                    handed(guest_landed.at[pl.ds(0, folded), pl.ds(0, in_two)], guest_sum_send)
                    handed(guest_landed.at[pl.ds(0, slices), pl.ds(0, at_once)], guest_direct)

                pl.when(boss)(lambda: guests_left(parts - 1, peers - 1))
                pl.when(other)(lambda: guests_left(parts, peers))
                pltpu.make_async_copy(summed, summed, back_send).wait()


def solution(mesh):
    parts, line, peers = mesh.shape["grp"], mesh.shape["fs"], mesh.shape["tp"]

    def local(*arrays):
        rows, width = arrays[0].shape
        held, units = arrays[2].shape
        kept = rows // peers
        pairs = peers // parts
        lent = units * 6 // 11 // 128 * 128 if line >= 4 and peers > 1 else 0
        slices = 4 if held % 512 == 0 else 1
        thin = held // slices
        half, full = jnp.bfloat16, jnp.float32
        spans = (units - lent, lent) if lent else (units,)
        dma = pltpu.SemaphoreType.DMA
        scratch = [
            pltpu.VMEM((span // WIDE, 2, width, WIDE), half) for span in spans if span // WIDE
        ]
        scratch += [pltpu.VMEM((2, width, span % WIDE), half) for span in spans if span % WIDE]
        scratch += [pltpu.VMEM((width, span), half) for span in spans]
        scratch += [pltpu.VMEM((rows, span), half) for span in spans]
        pieces = sum(pl.cdiv(span, WIDE) * CUT + slices for span in spans)
        scratch += [
            pltpu.VMEM((held, units), full),
            pltpu.VMEM((held, units), full),
            pltpu.VMEM((held, units), full),
            pltpu.VMEM((rows, width), half),
            pltpu.VMEM((rows, width), half),
            pltpu.VMEM((rows, width), half),
            pltpu.VMEM((8, units), full),
            pltpu.VMEM((2, width), full),
            pltpu.VMEM((line * slices, rows, thin), half),
            pltpu.VMEM((line * slices, peers, kept, thin), half),
            pltpu.VMEM((line * slices, rows, thin), half),
            dma((3 * len(spans), 3)),
            dma((pieces, line)),
            dma((2 * len(spans) + 2,)),
            dma((4,)),
            dma((2,)),
            dma,
            dma((line * slices,)),
            dma,
            dma((line * slices,)),
        ]
        if lent:
            scratch += [
                pltpu.VMEM((rows, width), half),
                pltpu.VMEM((rows, width), half),
                pltpu.VMEM((rows, lent), half),
                pltpu.VMEM((line * slices, rows, thin), half),
                pltpu.VMEM((line * slices, peers, kept, thin), half),
                pltpu.VMEM((line * slices, pairs, parts * kept, thin), half),
                pltpu.VMEM((line * slices, kept, thin), half),
                pltpu.VMEM((line * slices, kept, thin), half),
                dma((pairs + 1,)),
                dma((pairs,)),
                dma,
                dma((line * slices,)),
                dma,
                dma,
                dma((line * slices,)),
                dma,
                dma((line * slices,)),
            ]
        return pl.pallas_call(
            functools.partial(kernel, parts, line, peers, lent, slices),
            out_shape=pltpu.VMEM((kept, width), half),
            in_specs=[
                pl.BlockSpec(memory_space=pl.ANY if i in (0, 2, 3, 4) else pltpu.VMEM)
                for i in range(12)
            ],
            out_specs=pl.BlockSpec(memory_space=pltpu.VMEM),
            scratch_shapes=scratch,
            compiler_params=pltpu.CompilerParams(
                collective_id=0, has_side_effects=True, vmem_limit_bytes=62 * 1024 * 1024
            ),
        )(*arrays)

    return jax.shard_map(
        local,
        mesh=mesh,
        in_specs=(
            P(("grp", "fs"), None),
            P(),
            P("fs", "tp"),
            P("fs", "tp"),
            P("fs", "tp"),
            P("tp"),
            P("tp"),
            P(),
            P(None, "tp"),
            P(None, "tp"),
            P("tp"),
            P("tp"),
        ),
        out_specs=P(("grp", "fs", "tp"), None),
        check_vma=False,
    )
```
